32 devices in a mesh: ep: 4 (over y, x), tp: 8 (over z, core).
Axes of the slice: x: 2, y: 2, z: 4, core: 2. Of those that a mesh axis runs over, the one named last changes fastest.
Arguments:
- queries: bfloat16 [3072, 2048], P('ep', 'tp'), may hold values from -6 to 6
- keys: bfloat16 [3072, 512], P('ep'), may hold values from -6 to 6
- values: bfloat16 [3072, 512], P('ep'), may hold values from -6 to 6
- query_gain: float32 [128], replicated, may hold values from 1 to 4.5
- key_gain: float32 [128], replicated, may hold values from 1 to 4.5
- out_weight: bfloat16 [2048, 2048], P('tp'), may hold values from -0.75 to 0.75
- tokens_b: bfloat16 [1536, 2048], P('ep'), may hold values from -6 to 6
- norm_gain: float32 [2048], replicated, may hold values from 0.1 to 1.9
- routes: int32 [1536, 2], P('ep'), may hold values from 0 to 15, all different within a row; in each aligned block of 48 rows (0 to 47, 48 to 95, ...) at most 8 rows name the same one
- route_weight: float32 [1536, 2], P('ep'), may hold values from 0.2 to 1
- gate_weight: bfloat16 [16, 2048, 4096], P('ep', None, 'tp'), may hold values from -0.125 to 0.125
- up_weight: bfloat16 [16, 2048, 4096], P('ep', None, 'tp'), may hold values from -0.125 to 0.125
- down_weight: bfloat16 [16, 4096, 2048], P('ep', 'tp'), may hold values from -0.09375 to 0.09375
Outputs:
- mixed_out: bfloat16 [3072, 2048], P(('ep', 'tp'))
- expert_out: bfloat16 [1536, 2048], P(('ep', 'tp'))
The draws below stay inside these ranges and needn't reach their ends.
Inputs may be any that keep to these rules, and one draw needn't show every extreme that they name: `routes`: A row names 2 different experts. In each aligned block of 48 rows no expert is named more than 8 times, a bound that some block reaches.
All inputs are finite; a program needn't handle non-finite values.
Results may differ from the reference program's by a relative error of at most 0.019.
Values may be sent and summed in bfloat16 or wider, within the bound.
No kernel may reach another device: no remote copies, remote signals or barrier semaphores. Data moves between devices by JAX's collectives and lax.ppermute only.
A program may use at most 128 MiB of HBM per device.

```python
import math
import jax
import jax.numpy as jnp
import numpy as np
from jax import lax

D = 2048
HD = 128
HQ = 16
KVH = 4
GROUP = 4
FF = 4096
EXPERTS = 16
TOPK = 2
GRID_W = 64
TOK_DEV = 48
CAP = 8
LEN = 3072
TOKB = 1536
N_TP = 8


def draw_queries(key, part):
    drawn = jax.random.normal(jax.random.fold_in(key, 11), (LEN, HQ, HD), jnp.float32)
    return jnp.clip(drawn, -6.0, 6.0).reshape(LEN, HQ * HD).astype(jnp.bfloat16)


def draw_keys(key, part):
    drawn = jax.random.normal(jax.random.fold_in(key, 12), (LEN, KVH, HD), jnp.float32)
    return jnp.clip(drawn, -6.0, 6.0).reshape(LEN, KVH * HD).astype(jnp.bfloat16)


def draw_query_gain(key, part):
    uniform_g = jax.random.uniform(jax.random.fold_in(key, 13), (HD,), jnp.float32, 1.0, 2.0)
    return uniform_g


def draw_key_gain(key, part):
    uniform_g = jax.random.uniform(jax.random.fold_in(key, 14), (HD,), jnp.float32, 1.0, 2.0)
    return uniform_g


def block_scale(key, dims, pieces, smallest, top_value):
    level, own = 1.0, jax.random.fold_in(key, 6)
    for position, shards_of in pieces:
        steps = jnp.exp(jax.random.uniform(jax.random.fold_in(own, position), (shards_of,), jnp.float32, smallest / len(pieces), top_value / len(pieces)))
        level = level * jnp.repeat(steps, dims[position] // shards_of).reshape([-1 if axis == position else 1 for axis in range(len(dims))])
    return level


def deal_out(rng, own, number, rows, count, top, most, lean):
    sequence = jax.random.permutation(rng, count)
    heavy_load, common = load_shares(count, rows * top, most, lean, True), load_shares(count, rows * top, most, lean, False)
    places = jnp.arange(count)

    def named(sizes, rotation):
        used = int((sizes > 0).sum())
        fixed = max(1, used // 4)
        moved = fixed + (places - fixed + rotation * (used - fixed)) % max(1, count - fixed)
        return jnp.zeros((count,), jnp.int32).at[sequence[jnp.where(places < fixed, places, moved)]].set(jnp.asarray(sizes, jnp.int32))

    sizes = jnp.where(number % 4 == 0, named(heavy_load, number // 4), named(common, number - number // 4 - 1))
    mixed = jax.random.permutation(jax.random.fold_in(own, 3), count)
    donor, sink = mixed[0:count // 2 * 2:2], mixed[1:count // 2 * 2:2]
    room = jnp.minimum(sizes[donor] - 1, most - sizes[sink]) // 2
    room = jnp.where((donor == sequence[0]) | (sink == sequence[0]) | (sizes[sink] == 0), 0, jnp.maximum(room, 0))
    moved = jax.random.randint(jax.random.fold_in(own, 4), (count // 2,), 0, 1 << 20) % (room + 1)
    sizes = sizes.at[donor].add(-moved).at[sink].add(moved)
    labels = jnp.searchsorted(jnp.cumsum(sizes), jnp.arange(rows * top), side="right").astype(jnp.int32)
    table = labels.reshape(top, rows).T
    table = table[jax.random.permutation(jax.random.fold_in(own, 1), rows)]
    rotation = jax.random.randint(jax.random.fold_in(own, 2), (rows, 1), 0, top)
    return jnp.take_along_axis(table, (jnp.arange(top)[None, :] + rotation) % top, axis=1)


def load_shares(amount, total, most, slope, full):
    weights = [(1 << 20) // math.isqrt(grade ** slope) + 1 for grade in range(1, amount + 1)]
    largest = most if full else min(most, max(-(-total // amount), total * weights[0] // sum(weights)))
    least = 1 if total - largest >= amount - 1 else 0
    counts, rest = [largest] + [least] * (amount - 1), total - largest - least * (amount - 1)
    while rest > 0:
        movable = [i for i in range(1, amount) if counts[i] < largest] or [i for i in range(1, amount) if counts[i] < most]
        pool, budget = sum([weights[i] for i in movable]), rest
        for i in movable:
            extra = min(most - counts[i], max(1, budget * weights[i] // pool), rest)
            counts[i] = counts[i] + extra
            rest = rest - extra
    return np.array(counts)


def noise(own_key, shape, deviation, limit, pieces=(), kind=jnp.bfloat16):
    entries = jax.random.normal(own_key, shape, jnp.float32) * deviation
    if len(pieces) > 0:
        entries = block_scale(own_key, shape, pieces, -0.22, 0.18) * entries
    return jnp.clip(entries, min=-limit, max=limit).astype(kind)


def setup_inputs(seed: int = 0) -> dict:
    arg_keys = jax.random.split(jax.random.key(seed), 14)
    queries = draw_queries(jax.random.fold_in(arg_keys[13], 71), 0)
    keys = draw_keys(jax.random.fold_in(arg_keys[13], 71), 0)
    values = noise(arg_keys[2], (LEN, KVH * HD), 1.0, 6.0, ((0, 4),))
    query_gain = draw_query_gain(jax.random.fold_in(arg_keys[13], 71), 0)
    key_gain = draw_key_gain(jax.random.fold_in(arg_keys[13], 71), 0)
    out_weight = noise(arg_keys[5], (HQ * HD, D), (HD // 2) ** -0.5, 0.75, ((0, 8),))
    tokens_b = noise(arg_keys[6], (TOKB, D), 1.0, 6.0, ((0, 4),))
    norm_gain = jnp.clip(1.0 + 0.18 * jax.random.normal(arg_keys[7], (D,), jnp.float32), 0.1, 1.9)
    routes_keys = jax.random.split(jax.random.fold_in(arg_keys[8], 1), TOKB // TOK_DEV)
    routes_turns = jax.random.permutation(jax.random.fold_in(arg_keys[8], 3), TOKB // TOK_DEV)
    routes = jax.vmap(lambda own, number: deal_out(jax.random.fold_in(arg_keys[8], 2), own, number, TOK_DEV, EXPERTS, TOPK, CAP, 1))(routes_keys, routes_turns).reshape((TOKB, TOPK))
    route_weight = jnp.clip(jnp.exp(math.log(1.0) - 1.609438 * jax.random.uniform(arg_keys[9], (TOKB, TOPK), jnp.float32) ** block_scale(arg_keys[9], (TOKB, TOPK), ((0, 4),), -0.2, 0.2)), 0.2, 1.0)
    gate_weight = noise(arg_keys[10], (EXPERTS, D, FF), D ** -0.5, 0.125, ((0, 4), (2, 8)))
    up_weight = noise(arg_keys[11], (EXPERTS, D, FF), D ** -0.5, 0.125, ((0, 4), (2, 8)))
    down_weight = noise(arg_keys[12], (EXPERTS, FF, D), FF ** -0.5, 0.09375, ((0, 4), (1, 8)))
    return dict(queries=queries, keys=keys, values=values, query_gain=query_gain, key_gain=key_gain, out_weight=out_weight, tokens_b=tokens_b, norm_gain=norm_gain, routes=routes, route_weight=route_weight, gate_weight=gate_weight, up_weight=up_weight, down_weight=down_weight)


EPS = 1e-06
THETA = 10000.0
q_block = 64

def rotate(field, positions):
    n_freq = HD // 4
    row_pos = (positions // GRID_W).astype(jnp.float32)
    col_pos = (positions % GRID_W).astype(jnp.float32)
    inverse = THETA ** (-jnp.arange(n_freq, dtype=jnp.float32) / n_freq)
    angles = jnp.stack([row_pos[:, None] * inverse, col_pos[:, None] * inverse], axis=1)
    cosine = jnp.cos(angles)[:, None]
    sine = jnp.sin(angles)[:, None]
    length, n_heads = (field.shape[0], field.shape[1])
    halves = field.reshape(length, n_heads, 2, 2, n_freq)
    leading = halves[..., 0, :]
    second = halves[..., 1, :]
    turned = jnp.stack([leading * cosine - second * sine, second * cosine + leading * sine], axis=-2)
    return turned.reshape(length, n_heads, HD)

def prepare(source, gain_vec, positions, n_heads):
    length = source.shape[0]
    field = source.astype(jnp.float32).reshape(length, n_heads, HD)
    field = field * lax.rsqrt(lax.optimization_barrier(jnp.mean(field * field, axis=-1, keepdims=True)) + EPS) * gain_vec.astype(jnp.float32)
    return rotate(field, positions).astype(jnp.bfloat16)

def attend_block(query_blk, key_t, value_h):
    scores = jnp.einsum('qkgd,skd->kgqs', query_blk.astype(jnp.float32), key_t.astype(jnp.float32)) * HD ** (-0.5)
    row_max = lax.optimization_barrier(jnp.max(scores, axis=-1, keepdims=True))
    weights = jnp.exp(scores - row_max)
    totals = lax.optimization_barrier(jnp.sum(weights, axis=-1, keepdims=True))
    rounded = lax.optimization_barrier(weights.astype(jnp.bfloat16))
    merged = jnp.einsum('kgqs,skd->kgqd', rounded.astype(jnp.float32), value_h.astype(jnp.float32)) / totals
    return jnp.transpose(merged, (2, 0, 1, 3)).reshape(query_blk.shape[0], HQ * HD).astype(jnp.bfloat16)

def reference(queries, keys, values, query_gain, key_gain, out_weight, tokens_b, norm_gain, routes, route_weight, gate_weight, up_weight, down_weight):
    positions = jnp.arange(LEN, dtype=jnp.int32)
    query_t = prepare(queries, query_gain, positions, HQ).reshape(LEN // q_block, q_block, KVH, GROUP, HD)
    key_t = prepare(keys, key_gain, positions, KVH)
    value_h = values.reshape(LEN, KVH, HD)
    attended = lax.map(lambda query_blk: attend_block(query_blk, key_t, value_h), query_t).reshape(LEN, HQ * HD)
    mixed_out = jnp.dot(attended, out_weight, preferred_element_type=jnp.float32).astype(jnp.bfloat16)
    n_tokens = tokens_b.shape[0]
    n_blocks = n_tokens // TOK_DEV
    field = tokens_b.astype(jnp.float32)
    normed = (field * lax.rsqrt(lax.optimization_barrier(jnp.mean(field * field, axis=-1, keepdims=True)) + EPS) * norm_gain.astype(jnp.float32)).astype(jnp.bfloat16)
    assigned = routes.reshape(n_blocks, TOK_DEV * TOPK)
    onehot = (assigned[:, :, None] == jnp.arange(EXPERTS, dtype=jnp.int32)[None, None, :]).astype(jnp.int32)
    slot_rank = lax.optimization_barrier(jnp.sum((jnp.cumsum(onehot, axis=1) - onehot) * onehot, axis=-1))
    block_ids = jnp.arange(n_blocks, dtype=jnp.int32)[:, None]
    flat_slot = ((assigned * n_blocks + block_ids) * CAP + slot_rank).reshape(-1).astype(jnp.int32)
    row_ids = (block_ids * TOK_DEV + jnp.arange(TOK_DEV * TOPK, dtype=jnp.int32)[None, :] // TOPK).reshape(-1).astype(jnp.int32)
    slot_table = jnp.full((EXPERTS * n_blocks * CAP,), n_tokens, jnp.int32).at[flat_slot].set(row_ids)
    padded = jnp.concatenate([normed, jnp.zeros((1, D), jnp.bfloat16)], axis=0)
    width_part = FF // N_TP

    def expert_rows(stacked):
        row_index, gate_w, up_w, down_w = stacked
        inputs = padded[row_index].astype(jnp.float32)
        gate_act = jnp.einsum('nd,dtf->tnf', inputs, gate_w.reshape(D, N_TP, width_part).astype(jnp.float32))
        up_act = jnp.einsum('nd,dtf->tnf', inputs, up_w.reshape(D, N_TP, width_part).astype(jnp.float32))
        hidden = lax.optimization_barrier((jax.nn.silu(gate_act) * up_act).astype(jnp.bfloat16))
        partial_value = jnp.einsum('tnf,tfd->tnd', hidden.astype(jnp.float32), down_w.reshape(N_TP, width_part, D).astype(jnp.float32))
        partial_value = lax.optimization_barrier(partial_value.astype(jnp.bfloat16))
        return lax.optimization_barrier(jnp.sum(partial_value.astype(jnp.float32), axis=0)).astype(jnp.bfloat16)
    results = lax.map(expert_rows, (slot_table.reshape(EXPERTS, n_blocks * CAP), gate_weight, up_weight, down_weight))
    picked = results.reshape(-1, D)[flat_slot].astype(jnp.float32).reshape(n_tokens, TOPK, D)
    shares = route_weight / lax.optimization_barrier(jnp.sum(route_weight, axis=-1, keepdims=True))
    expert_out = lax.optimization_barrier(jnp.sum(shares[:, :, None] * picked, axis=1)).astype(jnp.bfloat16)
    return (mixed_out, expert_out)
```

```python
import jax
import jax.numpy as jnp
from jax import lax
from jax.experimental import pallas as pl
from jax.experimental.pallas import tpu as pltpu
from jax.sharding import Mesh, PartitionSpec as P

HD = 128
KVH = 4
EXPERTS = 16
TOPK = 2
GRID_W = 64
CAP = 8
EPS = 1e-06
THETA = 10000.0
CORES = 2
MIB = 1024 * 1024

F32 = jnp.float32
BF16 = jnp.bfloat16


def rope_tables(positions):
    n_freq = HD // 4
    row_pos = (positions // GRID_W).astype(F32)[:, None]
    col_pos = (positions % GRID_W).astype(F32)[:, None]
    lane = jnp.arange(HD, dtype=jnp.int32)
    inverse = THETA ** (-(lane % n_freq).astype(F32) / n_freq)
    angle = jnp.where(lane < HD // 2, row_pos, col_pos) * inverse
    sign = jnp.where((lane // n_freq) % 2 == 0, -1.0, 1.0).astype(F32)
    return jnp.cos(angle), jnp.sin(angle) * sign


def norm_turn(field, gain, cosine, sine):
    quarter = HD // 4
    mean = jnp.mean(field * field, axis=-1, keepdims=True)
    field = field * lax.rsqrt(mean + EPS) * gain
    lane = lax.broadcasted_iota(jnp.int32, field.shape, 1)
    partner = jnp.where(
        (lane // quarter) % 2 == 0,
        pltpu.roll(field, HD - quarter, 1),
        pltpu.roll(field, quarter, 1),
    )
    return field * cosine + partner * sine


def kv_kernel(core_ref, head_ref, keys_ref, values_ref, gain_ref, cos_ref, sin_ref, out_ref):
    rows = cos_ref.shape[0]
    field = keys_ref[...].reshape(rows, HD).astype(F32)
    out_ref[0] = norm_turn(field, gain_ref[...], cos_ref[...], sin_ref[...]).astype(BF16)
    out_ref[1] = values_ref[...].reshape(rows, HD)


def prepare_kv(core, head, keys, values, gain, cosine, sine, n_z):
    rows = cosine.shape[0]
    part = rows // n_z
    view = lambda a: a.reshape(n_z, CORES, part, a.shape[-1])
    picked = pl.BlockSpec((n_z, 1, part, HD), lambda i, c, h: (0, c[0], 0, h[0]))
    whole = lambda shape: pl.BlockSpec(shape, lambda i, c, h: (0,) * len(shape))
    return pl.pallas_call(
        kv_kernel,
        grid_spec=pltpu.PrefetchScalarGridSpec(
            num_scalar_prefetch=2,
            grid=(1,),
            in_specs=[picked, picked, whole((1, HD)), whole((rows, HD)), whole((rows, HD))],
            out_specs=whole((2, rows, HD)),
        ),
        out_shape=jax.ShapeDtypeStruct((2, rows, HD), BF16),
        name="prepare_kv",
    )(core, head, view(keys), view(values), gain, cosine, sine)


def mix_kernel(n_pieces, core_ref, q_own, q_other, gain_ref, cos_ref, sin_ref, w_own, w_other, *rest):
    pieces = rest[:n_pieces]
    out_ref, att_ref, keys_ref, vals_ref = rest[n_pieces:]
    rows = cos_ref.shape[0]
    row = 0
    for piece in pieces:
        for n in range(piece.shape[0]):
            keys_ref[pl.ds(row, rows)] = piece[n, 0]
            vals_ref[pl.ds(row, rows)] = piece[n, 1]
            row += rows
    factor = HD ** (-0.5) * 1.4426950408889634
    heads = q_own.shape[-1] // HD
    for source, field_ref in enumerate((q_own, q_other)):
        for head in range(heads):
            field = field_ref[:, :, :, head * HD : (head + 1) * HD].reshape(rows, HD).astype(F32)
            query = norm_turn(field, gain_ref[...], cos_ref[...], sin_ref[...]).astype(BF16)
            scores = lax.dot_general(
                query, keys_ref[...], (((1,), (1,)), ((), ())), preferred_element_type=F32
            )
            top = jnp.max(scores, axis=1, keepdims=True)
            weights = jnp.exp2((scores - top) * factor)
            totals = jnp.sum(weights, axis=1, keepdims=True)
            merged = jnp.dot(weights.astype(BF16), vals_ref[...], preferred_element_type=F32)
            at = (source * heads + head) * HD
            att_ref[:, at : at + HD] = (merged / totals).astype(BF16)
    half = heads * HD
    mixed = jnp.dot(att_ref[:, :half], w_own[...], preferred_element_type=F32)
    mixed = mixed + jnp.dot(att_ref[:, half:], w_other[...], preferred_element_type=F32)
    out_ref[...] = mixed.astype(BF16)


def mix(core, queries, q_other, gain, cosine, sine, w_own, w_other, pieces, n_z):
    rows, width = cosine.shape[0], queries.shape[-1]
    part = rows // n_z
    view = queries.reshape(n_z, CORES, part, width)
    d_model = w_own.shape[-1]
    length = sum(p.shape[0] for p in pieces) * rows
    whole = lambda a: pl.BlockSpec(a.shape, lambda i, c: (0,) * a.ndim)
    others = [q_other.reshape(n_z, 1, part, width), gain, cosine, sine, w_own, w_other, *pieces]
    return pl.pallas_call(
        lambda *refs: mix_kernel(len(pieces), *refs),
        grid_spec=pltpu.PrefetchScalarGridSpec(
            num_scalar_prefetch=1,
            grid=(1,),
            in_specs=[pl.BlockSpec((n_z, 1, part, width), lambda i, c: (0, c[0], 0, 0))]
            + [whole(a) for a in others],
            out_specs=pl.BlockSpec((rows, d_model), lambda i, c: (0, 0)),
            scratch_shapes=[
                pltpu.VMEM((rows, 2 * width), BF16),
                pltpu.VMEM((length, HD), BF16),
                pltpu.VMEM((length, HD), BF16),
            ],
        ),
        out_shape=jax.ShapeDtypeStruct((rows, d_model), BF16),
        compiler_params=pltpu.CompilerParams(vmem_limit_bytes=56 * MIB),
        name="mix",
    )(core, view, *others)


def dispatch_kernel(core_ref, tokens_ref, gain_ref, slots_ref, out_ref):
    rows, d_model = slots_ref.shape[-1], tokens_ref.shape[-1]
    field = tokens_ref[...].reshape(rows, d_model).astype(F32)
    mean = jnp.mean(field * field, axis=-1, keepdims=True)
    normed = (field * lax.rsqrt(mean + EPS) * gain_ref[...]).astype(BF16)
    slot = lax.broadcasted_iota(jnp.int32, (out_ref.shape[0], rows), 0)
    hot = slot == slots_ref[0:1]
    for k in range(1, TOPK):
        hot = hot | (slot == slots_ref[k : k + 1])
    out_ref[...] = jnp.dot(
        hot.astype(F32).astype(BF16), normed, preferred_element_type=F32
    ).astype(BF16)


def dispatch(core, tokens, gain, slots, n_z):
    local_rows, d_model = tokens.shape
    part = local_rows // (n_z * CORES)
    n_slots = EXPERTS * n_z * CAP
    return pl.pallas_call(
        dispatch_kernel,
        grid_spec=pltpu.PrefetchScalarGridSpec(
            num_scalar_prefetch=1,
            grid=(1,),
            in_specs=[
                pl.BlockSpec((n_z, 1, part, d_model), lambda i, c: (0, c[0], 0, 0)),
                pl.BlockSpec((1, d_model), lambda i, c: (0, 0)),
                pl.BlockSpec(slots.shape, lambda i, c: (0, 0)),
            ],
            out_specs=pl.BlockSpec((n_slots, d_model), lambda i, c: (0, 0)),
        ),
        out_shape=jax.ShapeDtypeStruct((n_slots, d_model), BF16),
        name="dispatch",
    )(core, tokens.reshape(n_z, CORES, part, d_model), gain, slots)


def expert_kernel(own_ref, other_ref, gate_ref, up_ref, down_ref, keep_ref, send_ref, acc_ref):
    step = pl.program_id(1)
    n_src, _, rows, d_model = own_ref.shape
    half = n_src * rows
    field = jnp.concatenate(
        [own_ref[...].reshape(half, d_model), other_ref[...].reshape(half, d_model)], axis=0
    )
    gate = jnp.dot(field, gate_ref[0], preferred_element_type=F32)
    up = jnp.dot(field, up_ref[0], preferred_element_type=F32)
    hidden = (gate / (1.0 + jnp.exp(-gate)) * up).astype(BF16)
    result = jnp.dot(hidden, down_ref[0], preferred_element_type=F32)

    @pl.when(step == 0)
    def _():
        acc_ref[...] = result

    @pl.when(step > 0)
    def _():
        acc_ref[...] += result

    @pl.when(step == pl.num_programs(1) - 1)
    def _():
        keep_ref[...] = acc_ref[:half].astype(BF16).reshape(keep_ref.shape)
        send_ref[...] = acc_ref[half:].astype(BF16).reshape(send_ref.shape)


def experts(own, other, gate_weight, up_weight, down_weight):
    n_src, n_local, rows, d_model = own.shape
    width = gate_weight.shape[-1]
    steps = 2 if width % 512 == 0 else 1
    cut = width // steps
    act = pl.BlockSpec((n_src, 1, rows, d_model), lambda e, s: (0, e, 0, 0))
    return pl.pallas_call(
        expert_kernel,
        grid=(n_local, steps),
        in_specs=[
            act,
            act,
            pl.BlockSpec((1, d_model, cut), lambda e, s: (e, 0, s)),
            pl.BlockSpec((1, d_model, cut), lambda e, s: (e, 0, s)),
            pl.BlockSpec((1, cut, d_model), lambda e, s: (e, s, 0)),
        ],
        out_specs=[act, act],
        out_shape=[jax.ShapeDtypeStruct(own.shape, BF16)] * 2,
        scratch_shapes=[pltpu.VMEM((2 * n_src * rows, d_model), F32)],
        compiler_params=pltpu.CompilerParams(vmem_limit_bytes=40 * MIB),
        name="experts",
    )(own, other, gate_weight, up_weight, down_weight)


def combine_kernel(slots_ref, shares_ref, back_ref, out_ref):
    rows, n_slots = slots_ref.shape[0], back_ref.shape[0]
    slot = lax.broadcasted_iota(jnp.int32, (rows, n_slots), 1)
    matrix = jnp.zeros((rows, n_slots), F32)
    for k in range(TOPK):
        matrix = matrix + jnp.where(slot == slots_ref[:, k : k + 1], shares_ref[:, k : k + 1], 0.0)
    high = matrix.astype(BF16)
    low = (matrix - high.astype(F32)).astype(BF16)
    back = back_ref[...]
    out_ref[...] = (
        jnp.dot(high, back, preferred_element_type=F32)
        + jnp.dot(low, back, preferred_element_type=F32)
    ).astype(BF16)


def combine(slots, shares, back):
    return pl.pallas_call(
        combine_kernel,
        out_shape=jax.ShapeDtypeStruct((slots.shape[0], back.shape[-1]), BF16),
        name="combine",
    )(slots, shares, back)


def swap_cores(a):
    return lax.ppermute(a, "core", [(i, CORES - 1 - i) for i in range(CORES)])


def on_device(
    queries,
    keys,
    values,
    query_gain,
    key_gain,
    out_weight,
    tokens_b,
    norm_gain,
    routes,
    route_weight,
    gate_weight,
    up_weight,
    down_weight,
):
    n_ep, n_z = lax.axis_size("ep"), lax.axis_size("z")
    core, z_index = lax.axis_index("core"), lax.axis_index("z")
    core_arg = core.reshape(1).astype(jnp.int32)
    other_arg = 1 - core_arg
    n_rows, width = queries.shape
    d_model = tokens_b.shape[-1]
    heads = width // HD
    n_heads = heads * n_z * CORES

    part = n_rows // (n_z * CORES)
    offsets = (
        jnp.arange(n_z, dtype=jnp.int32)[:, None] * (CORES * part)
        + core * part
        + jnp.arange(part, dtype=jnp.int32)[None, :]
    ).reshape(-1)
    cosine, sine = rope_tables(lax.axis_index("ep") * n_rows + offsets)
    kv_head = ((z_index * CORES + core) * heads // (n_heads // KVH)).reshape(1).astype(jnp.int32)
    own_kv = prepare_kv(core_arg, kv_head, keys, values, key_gain[None], cosine, sine, n_z)
    if n_ep <= 4:
        mine = [own_kv[None]]
        for step in range(1, n_ep):
            mine.append(
                lax.ppermute(own_kv, "ep", [(i, (i + step) % n_ep) for i in range(n_ep)])[None]
            )
        gathered = jnp.concatenate(mine, axis=0)
    else:
        gathered = lax.all_gather(own_kv, "ep", axis=0, tiled=False)
    other_kv = swap_cores(gathered)

    q_view = queries.reshape(n_z, CORES, part, width)
    q_other = swap_cores(lax.dynamic_index_in_dim(q_view, 1 - core, 1, keepdims=False))
    w_other = swap_cores(out_weight)

    block_rows = tokens_b.shape[0] // (n_z * CORES)
    picks = block_rows * TOPK
    own_block = lambda a: lax.dynamic_index_in_dim(
        a.reshape(n_z, CORES, block_rows, TOPK), core, 1, keepdims=False
    )
    own_routes = own_block(routes)
    assigned = own_routes.reshape(n_z, picks)
    earlier = jnp.arange(picks)[:, None] > jnp.arange(picks)[None, :]
    same = (assigned[:, :, None] == assigned[:, None, :]) & earlier[None]
    rank = jnp.sum(same.astype(jnp.int32), axis=-1)
    block = jnp.arange(n_z, dtype=jnp.int32)[:, None]
    slots = ((assigned * n_z + block) * CAP + rank).reshape(n_z * block_rows, TOPK)
    own_weight = own_block(route_weight).reshape(n_z * block_rows, TOPK)
    shares = own_weight / jnp.sum(own_weight, axis=-1, keepdims=True)

    outgoing = dispatch(core_arg, tokens_b, norm_gain[None], slots.T, n_z)
    n_local = gate_weight.shape[0]
    outgoing = outgoing.reshape(n_ep, n_local, n_z * CAP, d_model)
    arrived = lax.all_to_all(outgoing, "ep", split_axis=0, concat_axis=0, tiled=True)
    arrived_other = swap_cores(arrived)

    mixed = mix(
        core_arg, queries, q_other, query_gain[None], cosine, sine, out_weight, w_other,
        [gathered, other_kv], n_z,
    )
    mixed = lax.all_to_all(
        mixed.reshape(n_z, part, d_model), "z", split_axis=0, concat_axis=0, tiled=True
    )
    mixed_out = jnp.sum(mixed.astype(F32), axis=0).astype(BF16)

    keep, send = experts(arrived, arrived_other, gate_weight, up_weight, down_weight)
    result = (keep.astype(F32) + swap_cores(send).astype(F32)).astype(BF16)
    back = lax.all_to_all(result, "ep", split_axis=0, concat_axis=0, tiled=True)
    rows = combine(slots, shares, back.reshape(-1, d_model))
    rows = lax.all_to_all(
        rows.reshape(n_z, block_rows, d_model), "z", split_axis=0, concat_axis=0, tiled=True
    )
    expert_out = jnp.sum(rows.astype(F32), axis=0).astype(BF16)
    return (mixed_out, expert_out)


def solution(mesh):
    n_ep, n_tp = mesh.shape["ep"], mesh.shape["tp"]
    fine = Mesh(mesh.devices.reshape(n_ep, n_tp // CORES, CORES), ("ep", "z", "core"))
    tp = ("z", "core")
    placed = (
        P("ep", tp),
        P("ep", None),
        P("ep", None),
        P(),
        P(),
        P(tp, None),
        P("ep", None),
        P(),
        P("ep", None),
        P("ep", None),
        P("ep", None, tp),
        P("ep", None, tp),
        P("ep", tp, None),
    )
    return jax.shard_map(
        on_device,
        mesh=fine,
        in_specs=placed,
        out_specs=(P(("ep", "z", "core"), None), P(("ep", "z", "core"), None)),
        check_vma=False,
    )
```

```python
import jax
import jax.numpy as jnp
from jax import lax
from jax.experimental import pallas as pl
from jax.experimental.pallas import tpu as pltpu
from jax.sharding import Mesh, PartitionSpec as P


HD = 128
KVH = 4
EXPERTS = 16
TOPK = 2
GRID_W = 64
CAP = 8
EPS = 1e-06
THETA = 10000.0
CORES = 2
MIB = 1024 * 1024

F32 = jnp.float32
BF16 = jnp.bfloat16


def rope_tables(positions):
    n_freq = HD // 4
    row_pos = (positions // GRID_W).astype(F32)[:, None]
    col_pos = (positions % GRID_W).astype(F32)[:, None]
    lane = jnp.arange(HD, dtype=jnp.int32)
    inverse = THETA ** (-(lane % n_freq).astype(F32) / n_freq)
    angle = jnp.where(lane < HD // 2, row_pos, col_pos) * inverse
    sign = jnp.where((lane // n_freq) % 2 == 0, -1.0, 1.0).astype(F32)
    return jnp.cos(angle), jnp.sin(angle) * sign


def norm_turn(field, gain, cosine, sine):
    quarter = HD // 4
    mean = jnp.mean(field * field, axis=-1, keepdims=True)
    field = field * lax.rsqrt(mean + EPS) * gain
    lane = lax.broadcasted_iota(jnp.int32, field.shape, 1)
    partner = jnp.where(
        (lane // quarter) % 2 == 0,
        pltpu.roll(field, HD - quarter, 1),
        pltpu.roll(field, quarter, 1),
    )
    return field * cosine + partner * sine


def kv_kernel(core_ref, head_ref, keys_ref, values_ref, gain_ref, cos_ref, sin_ref, out_ref):
    rows = cos_ref.shape[0]
    field = keys_ref[...].reshape(rows, HD).astype(F32)
    out_ref[0] = norm_turn(field, gain_ref[...], cos_ref[...], sin_ref[...]).astype(BF16)
    out_ref[1] = values_ref[...].reshape(rows, HD)


def prepare_kv(core, head, keys, values, gain, cosine, sine, n_z):
    rows = cosine.shape[0]
    part = rows // n_z
    view = lambda a: a.reshape(n_z, CORES, part, a.shape[-1])
    picked = pl.BlockSpec((n_z, 1, part, HD), lambda i, c, h: (0, c[0], 0, h[0]))
    whole = lambda shape: pl.BlockSpec(shape, lambda i, c, h: (0,) * len(shape))
    return pl.pallas_call(
        kv_kernel,
        grid_spec=pltpu.PrefetchScalarGridSpec(
            num_scalar_prefetch=2,
            grid=(1,),
            in_specs=[picked, picked, whole((1, HD)), whole((rows, HD)), whole((rows, HD))],
            out_specs=whole((2, rows, HD)),
        ),
        out_shape=jax.ShapeDtypeStruct((2, rows, HD), BF16),
        name="prepare_kv",
    )(core, head, view(keys), view(values), gain, cosine, sine)


def mix_kernel(n_pieces, n_out, core_ref, z_ref, q_own, q_other, gain_ref, cos_ref, sin_ref, *rest):
    w_own, w_other = rest[:2]
    pieces = rest[2 : 2 + n_pieces]
    outs = rest[2 + n_pieces : 2 + n_pieces + n_out]
    keys_ref, vals_ref = rest[2 + n_pieces + n_out :]
    step = pl.program_id(0)

    @pl.when(step == 0)
    def _():
        row = 0
        for piece in pieces:
            rows = piece.shape[1]
            keys_ref[pl.ds(row, rows)] = piece[0]
            vals_ref[pl.ds(row, rows)] = piece[1]
            row += rows

    factor = HD ** (-0.5) * 1.4426950408889634
    part = cos_ref.shape[0]
    heads = q_own.shape[-1] // HD
    queries = []
    for field in (q_own[...].reshape(part, heads * HD), q_other[0]):
        for head in range(heads):
            one = field[:, head * HD : (head + 1) * HD].astype(F32)
            queries.append(norm_turn(one, gain_ref[...], cos_ref[...], sin_ref[...]).astype(BF16))
    query = jnp.concatenate(queries, axis=0)
    scores = lax.dot_general(
        query, keys_ref[...], (((1,), (1,)), ((), ())), preferred_element_type=F32
    )
    top = jnp.max(scores, axis=1, keepdims=True)
    weights = jnp.exp2((scores - top) * factor)
    totals = jnp.sum(weights, axis=1, keepdims=True)
    merged = jnp.dot(weights.astype(BF16), vals_ref[...], preferred_element_type=F32)
    merged = (merged / totals).astype(BF16)
    sides = []
    for side in range(2):
        picked = [merged[(side * heads + h) * part : (side * heads + h + 1) * part] for h in range(heads)]
        sides.append(jnp.concatenate(picked, axis=1) if heads > 1 else picked[0])
    mixed = jnp.dot(sides[0], w_own[...], preferred_element_type=F32)
    mixed = mixed + jnp.dot(sides[1], w_other[...], preferred_element_type=F32)
    mixed = mixed.astype(BF16)
    for n, out_ref in enumerate(outs):

        @pl.when(step == n)
        def _():
            out_ref[...] = mixed


def mix(core, z_index, queries, q_other, gain, cosine, sine, w_own, w_other, pieces, n_z):
    rows, width = cosine.shape[0], queries.shape[-1]
    part = rows // n_z
    d_model = w_own.shape[-1]
    length = sum(p.shape[1] for p in pieces)
    whole = lambda a: pl.BlockSpec(a.shape, lambda i, c, z: (0,) * a.ndim)
    turn = lambda i, z: lax.rem(i + z[0], n_z)
    table = pl.BlockSpec((part, HD), lambda i, c, z: (turn(i, z), 0))
    return pl.pallas_call(
        lambda *refs: mix_kernel(len(pieces), n_z, *refs),
        grid_spec=pltpu.PrefetchScalarGridSpec(
            num_scalar_prefetch=2,
            grid=(n_z,),
            in_specs=[
                pl.BlockSpec((1, 1, part, width), lambda i, c, z: (turn(i, z), c[0], 0, 0)),
                pl.BlockSpec((1, part, width), lambda i, c, z: (turn(i, z), 0, 0)),
                whole(gain),
                table,
                table,
                whole(w_own),
                whole(w_other),
            ]
            + [whole(p) for p in pieces],
            out_specs=[pl.BlockSpec((part, d_model), lambda i, c, z: (0, 0))] * n_z,
            scratch_shapes=[pltpu.VMEM((length, HD), BF16), pltpu.VMEM((length, HD), BF16)],
        ),
        out_shape=[jax.ShapeDtypeStruct((part, d_model), BF16)] * n_z,
        compiler_params=pltpu.CompilerParams(vmem_limit_bytes=56 * MIB),
        name="mix",
    )(
        core, z_index, queries.reshape(n_z, CORES, part, width), q_other, gain, cosine, sine,
        w_own, w_other, *pieces,
    )


def dispatch_kernel(core_ref, tokens_ref, gain_ref, slots_ref, *out_refs):
    rows, d_model = slots_ref.shape[-1], tokens_ref.shape[-1]
    field = tokens_ref[...].reshape(rows, d_model).astype(F32)
    mean = jnp.mean(field * field, axis=-1, keepdims=True)
    normed = (field * lax.rsqrt(mean + EPS) * gain_ref[...]).astype(BF16)
    for chunk, out_ref in enumerate(out_refs):
        n_slots = out_ref.shape[0]
        slot = lax.broadcasted_iota(jnp.int32, (n_slots, rows), 0) + chunk * n_slots
        hot = slot == slots_ref[0:1]
        for k in range(1, TOPK):
            hot = hot | (slot == slots_ref[k : k + 1])
        out_ref[...] = jnp.dot(
            hot.astype(F32).astype(BF16), normed, preferred_element_type=F32
        ).astype(BF16)


def dispatch(core, tokens, gain, slots, n_z, pieces):
    local_rows, d_model = tokens.shape
    part = local_rows // (n_z * CORES)
    n_slots = EXPERTS * n_z * CAP // pieces
    return pl.pallas_call(
        dispatch_kernel,
        grid_spec=pltpu.PrefetchScalarGridSpec(
            num_scalar_prefetch=1,
            grid=(1,),
            in_specs=[
                pl.BlockSpec((n_z, 1, part, d_model), lambda i, c: (0, c[0], 0, 0)),
                pl.BlockSpec((1, d_model), lambda i, c: (0, 0)),
                pl.BlockSpec(slots.shape, lambda i, c: (0, 0)),
            ],
            out_specs=[pl.BlockSpec((n_slots, d_model), lambda i, c: (0, 0))] * pieces,
        ),
        out_shape=[jax.ShapeDtypeStruct((n_slots, d_model), BF16)] * pieces,
        name="dispatch",
    )(core, tokens.reshape(n_z, CORES, part, d_model), gain, slots)


def expert_kernel(n_src, *refs):
    ins, (gate_ref, up_ref, down_ref) = refs[: 2 * n_src], refs[2 * n_src : 2 * n_src + 3]
    outs, (field_ref, acc_ref) = refs[2 * n_src + 3 : -2], refs[-2:]
    step = pl.program_id(1)
    rows = ins[0].shape[1]

    @pl.when(step == 0)
    def _():
        for n, ref in enumerate(ins):
            field_ref[n * rows : (n + 1) * rows] = ref[0]

    field = field_ref[...]
    gate = jnp.dot(field, gate_ref[0], preferred_element_type=F32)
    up = jnp.dot(field, up_ref[0], preferred_element_type=F32)
    hidden = (gate / (1.0 + jnp.exp(-gate)) * up).astype(BF16)
    result = jnp.dot(hidden, down_ref[0], preferred_element_type=F32)

    @pl.when(step == 0)
    def _():
        acc_ref[...] = result

    @pl.when(step > 0)
    def _():
        acc_ref[...] += result

    @pl.when(step == pl.num_programs(1) - 1)
    def _():
        for n, ref in enumerate(outs):
            ref[0] = acc_ref[n * rows : (n + 1) * rows].astype(BF16)


def experts(own, other, gate_weight, up_weight, down_weight, first):
    pieces = [*own, *other]
    per, rows, d_model = pieces[0].shape
    width = gate_weight.shape[-1]
    steps = 2 if width % 512 == 0 else 1
    cut = width // steps
    act = pl.BlockSpec((1, rows, d_model), lambda e, s: (e, 0, 0))
    outs = pl.pallas_call(
        lambda *refs: expert_kernel(len(own), *refs),
        grid=(per, steps),
        in_specs=[act] * len(pieces)
        + [
            pl.BlockSpec((1, d_model, cut), lambda e, s: (e + first, 0, s)),
            pl.BlockSpec((1, d_model, cut), lambda e, s: (e + first, 0, s)),
            pl.BlockSpec((1, cut, d_model), lambda e, s: (e + first, s, 0)),
        ],
        out_specs=[act] * len(pieces),
        out_shape=[jax.ShapeDtypeStruct((per, rows, d_model), BF16)] * len(pieces),
        scratch_shapes=[
            pltpu.VMEM((len(pieces) * rows, d_model), BF16),
            pltpu.VMEM((len(pieces) * rows, d_model), F32),
        ],
        compiler_params=pltpu.CompilerParams(vmem_limit_bytes=40 * MIB),
        name="experts",
    )(*pieces, gate_weight, up_weight, down_weight)
    return outs[: len(own)], outs[len(own) :]


def combine_kernel(n_back, z_ref, slots_ref, shares_ref, *rest):
    back_refs, out_refs, total_ref = rest[:n_back], rest[n_back:-1], rest[-1]
    rows = slots_ref.shape[0]
    total = jnp.zeros((rows, back_refs[0].shape[-1]), F32)
    for piece, back_ref in enumerate(back_refs):
        n_slots = back_ref.shape[0]
        slot = lax.broadcasted_iota(jnp.int32, (rows, n_slots), 1) + piece * n_slots
        matrix = jnp.zeros((rows, n_slots), F32)
        for k in range(TOPK):
            share = shares_ref[:, k : k + 1]
            matrix = matrix + jnp.where(slot == slots_ref[:, k : k + 1], share, 0.0)
        high = matrix.astype(BF16)
        low = (matrix - high.astype(F32)).astype(BF16)
        back = back_ref[...]
        total = total + jnp.dot(high, back, preferred_element_type=F32)
        total = total + jnp.dot(low, back, preferred_element_type=F32)
    total_ref[...] = total.reshape(total_ref.shape)
    n_z = len(out_refs)
    for n, out_ref in enumerate(out_refs):
        out_ref[...] = total_ref[lax.rem(z_ref[0] + n, n_z)].astype(BF16)


def combine(z_index, slots, shares, backs, n_z):
    rows, d_model = slots.shape[0], backs[0].shape[-1]
    whole = lambda a: pl.BlockSpec(a.shape, lambda i, z: (0,) * a.ndim)
    return pl.pallas_call(
        lambda *refs: combine_kernel(len(backs), *refs),
        grid_spec=pltpu.PrefetchScalarGridSpec(
            num_scalar_prefetch=1,
            grid=(1,),
            in_specs=[whole(a) for a in (slots, shares, *backs)],
            out_specs=[pl.BlockSpec((rows // n_z, d_model), lambda i, z: (0, 0))] * n_z,
            scratch_shapes=[pltpu.VMEM((n_z, rows // n_z, d_model), F32)],
        ),
        out_shape=[jax.ShapeDtypeStruct((rows // n_z, d_model), BF16)] * n_z,
        name="combine",
    )(z_index, slots, shares, *backs)


def shift(a, axis, step):
    n = lax.axis_size(axis)
    return lax.ppermute(a, axis, [(i, (i + step) % n) for i in range(n)])


def swap_cores(a):
    return lax.ppermute(a, "core", [(i, CORES - 1 - i) for i in range(CORES)])


def on_device(
    queries,
    keys,
    values,
    query_gain,
    key_gain,
    out_weight,
    tokens_b,
    norm_gain,
    routes,
    route_weight,
    gate_weight,
    up_weight,
    down_weight,
):
    n_ep, n_z = lax.axis_size("ep"), lax.axis_size("z")
    core, z_index = lax.axis_index("core"), lax.axis_index("z")
    core_arg = core.reshape(1).astype(jnp.int32)
    z_arg = z_index.reshape(1).astype(jnp.int32)
    n_rows, width = queries.shape
    d_model = tokens_b.shape[-1]
    heads = width // HD
    n_heads = heads * n_z * CORES

    part = n_rows // (n_z * CORES)
    offsets = (
        jnp.arange(n_z, dtype=jnp.int32)[:, None] * (CORES * part)
        + core * part
        + jnp.arange(part, dtype=jnp.int32)[None, :]
    ).reshape(-1)
    cosine, sine = rope_tables(lax.axis_index("ep") * n_rows + offsets)
    kv_head = ((z_index * CORES + core) * heads // (n_heads // KVH)).reshape(1).astype(jnp.int32)
    own_kv = prepare_kv(core_arg, kv_head, keys, values, key_gain[None], cosine, sine, n_z)
    pieces = [own_kv]
    for step in range(1, n_ep):
        pieces.append(shift(own_kv, "ep", step))
    pieces = pieces + [swap_cores(p) for p in pieces]

    q_view = queries.reshape(n_z, CORES, part, width)
    q_other = swap_cores(lax.dynamic_index_in_dim(q_view, 1 - core, 1, keepdims=False))
    w_other = swap_cores(out_weight)

    n_local = gate_weight.shape[0]
    chunks = 2 if n_local % 2 == 0 else 1
    per = n_local // chunks
    block_rows = tokens_b.shape[0] // (n_z * CORES)
    picks = block_rows * TOPK
    own_block = lambda a: lax.dynamic_index_in_dim(
        a.reshape(n_z, CORES, block_rows, TOPK), core, 1, keepdims=False
    )
    own_routes = own_block(routes)
    assigned = own_routes.reshape(n_z, picks)
    earlier = jnp.arange(picks)[:, None] > jnp.arange(picks)[None, :]
    same = (assigned[:, :, None] == assigned[:, None, :]) & earlier[None]
    rank = jnp.sum(same.astype(jnp.int32), axis=-1)
    block = jnp.arange(n_z, dtype=jnp.int32)[:, None]
    local = assigned % n_local
    ahead = lax.rem(assigned // n_local + n_ep - lax.axis_index("ep"), n_ep)
    place = ((local // per) * n_ep + ahead) * per + local % per
    slots = ((place * n_z + block) * CAP + rank).reshape(n_z * block_rows, TOPK)
    own_weight = own_block(route_weight).reshape(n_z * block_rows, TOPK)
    shares = own_weight / jnp.sum(own_weight, axis=-1, keepdims=True)

    outgoing = dispatch(core_arg, tokens_b, norm_gain[None], slots.T, n_z, chunks * n_ep)
    arrived = []
    for chunk in range(chunks):
        here = []
        for step in range(n_ep):
            piece = outgoing[chunk * n_ep + step].reshape(per, n_z * CAP, d_model)
            here.append(shift(piece, "ep", step) if step else piece)
        arrived.append((here, [swap_cores(p) for p in here]))

    mixed = mix(
        core_arg, z_arg, queries, q_other, query_gain[None], cosine, sine, out_weight, w_other,
        pieces, n_z,
    )
    gathered = [mixed[0].astype(F32)]
    for step in range(1, n_z):
        gathered.append(shift(mixed[step], "z", step).astype(F32))
    mixed_out = sum(gathered).astype(BF16)

    backs = []
    for chunk in range(chunks):
        keep, send = experts(
            *arrived[chunk], gate_weight, up_weight, down_weight, chunk * per
        )
        for step in range(n_ep):
            there = swap_cores(send[step])
            result = (keep[step].astype(F32) + there.astype(F32)).astype(BF16)
            result = shift(result, "ep", n_ep - step) if step else result
            backs.append(result.reshape(-1, d_model))
    rows = combine(z_arg, slots, shares, backs, n_z)
    gathered = [rows[0].astype(F32)]
    for step in range(1, n_z):
        gathered.append(shift(rows[step], "z", step).astype(F32))
    expert_out = sum(gathered).astype(BF16)
    return (mixed_out, expert_out)


def solution(mesh):
    n_ep, n_tp = mesh.shape["ep"], mesh.shape["tp"]
    fine = Mesh(mesh.devices.reshape(n_ep, n_tp // CORES, CORES), ("ep", "z", "core"))
    tp = ("z", "core")
    placed = (
        P("ep", tp),
        P("ep", None),
        P("ep", None),
        P(),
        P(),
        P(tp, None),
        P("ep", None),
        P(),
        P("ep", None),
        P("ep", None),
        P("ep", None, tp),
        P("ep", None, tp),
        P("ep", tp, None),
    )

    return jax.shard_map(
        on_device,
        mesh=fine,
        in_specs=placed,
        out_specs=(P(("ep", "z", "core"), None), P(("ep", "z", "core"), None)),
        check_vma=False,
    )
```

```python
import jax
import jax.numpy as jnp
from jax import lax
from jax.experimental import pallas as pl
from jax.experimental.pallas import tpu as pltpu
from jax.sharding import Mesh, PartitionSpec as P


HD = 128
KVH = 4
EXPERTS = 16
TOPK = 2
GRID_W = 64
CAP = 8
EPS = 1e-06
THETA = 10000.0
CORES = 2
IN_VMEM = pl.BlockSpec(memory_space=pltpu.VMEM)
IN_SMEM = pl.BlockSpec(memory_space=pltpu.SMEM)
KEY_CHUNK = 1024
MIB = 1024 * 1024

F32 = jnp.float32
BF16 = jnp.bfloat16


def in_hbm(arrays):
    return [pltpu.with_memory_space_constraint(a, pltpu.HBM) for a in arrays]


def rope_tables(positions):
    n_freq = HD // 4
    row_pos = (positions // GRID_W).astype(F32)[:, None]
    col_pos = (positions % GRID_W).astype(F32)[:, None]
    lane = jnp.arange(HD, dtype=jnp.int32)
    inverse = THETA ** (-(lane % n_freq).astype(F32) / n_freq)
    angle = jnp.where(lane < HD // 2, row_pos, col_pos) * inverse
    sign = jnp.where((lane // n_freq) % 2 == 0, -1.0, 1.0).astype(F32)
    return jnp.cos(angle), jnp.sin(angle) * sign


def norm_turn(field, gain, cosine, sine):
    quarter = HD // 4
    mean = jnp.mean(field * field, axis=-1, keepdims=True)
    field = field * lax.rsqrt(mean + EPS) * gain
    lane = lax.broadcasted_iota(jnp.int32, field.shape, 1)
    partner = jnp.where(
        (lane // quarter) % 2 == 0,
        pltpu.roll(field, HD - quarter, 1),
        pltpu.roll(field, quarter, 1),
    )
    return field * cosine + partner * sine


def prepare_kernel(
    core_ref, head_ref, keys_ref, values_ref, q_ref, gain_ref, cos_ref, sin_ref, kv_ref, send_ref
):
    rows = cos_ref.shape[0]
    field = keys_ref[...].reshape(rows, HD).astype(F32)
    kv_ref[0] = norm_turn(field, gain_ref[...], cos_ref[...], sin_ref[...]).astype(BF16)
    kv_ref[1] = values_ref[...].reshape(rows, HD)
    send_ref[...] = q_ref[...].reshape(send_ref.shape)


def prepare(core, head, keys, values, queries, gain, cosine, sine, n_z):
    rows, width = cosine.shape[0], queries.shape[-1]
    part = rows // n_z
    view = lambda a: a.reshape(n_z, CORES, part, a.shape[-1])
    picked = pl.BlockSpec((n_z, 1, part, HD), lambda i, c, h: (0, c[0], 0, h[0]))
    whole = lambda shape: pl.BlockSpec(shape, lambda i, c, h: (0,) * len(shape))
    return pl.pallas_call(
        prepare_kernel,
        grid_spec=pltpu.PrefetchScalarGridSpec(
            num_scalar_prefetch=2,
            grid=(1,),
            in_specs=[
                picked,
                picked,
                pl.BlockSpec((n_z, 1, part, width), lambda i, c, h: (0, 1 - c[0], 0, 0)),
                whole((1, HD)),
                whole((rows, HD)),
                whole((rows, HD)),
            ],
            out_specs=[IN_VMEM, IN_VMEM],
        ),
        out_shape=[
            jax.ShapeDtypeStruct((2, rows, HD), BF16),
            jax.ShapeDtypeStruct((n_z, part, width), BF16),
        ],
        compiler_params=pltpu.CompilerParams(vmem_limit_bytes=8 * MIB),
        name="prepare",
    )(core, head, *in_hbm([view(keys), view(values), view(queries)]), gain, cosine, sine)


def add_kernel(*refs):
    total = refs[0][...].astype(F32)
    for ref in refs[1:-1]:
        total = total + ref[...].astype(F32)
    refs[-1][...] = total.astype(BF16)


def add(*arrays):
    return pl.pallas_call(
        add_kernel,
        in_specs=[IN_VMEM] * len(arrays),
        out_specs=IN_VMEM,
        out_shape=jax.ShapeDtypeStruct(arrays[0].shape, BF16),
        compiler_params=pltpu.CompilerParams(vmem_limit_bytes=8 * MIB),
        name="add",
    )(*arrays)


def mix_kernel(n_pieces, n_z, core_ref, z_ref, q_own, q_other, gain_ref, cos_ref, sin_ref, *rest):
    w_own, w_other = rest[:2]
    pieces = rest[2 : 2 + n_pieces]
    outs = rest[2 + n_pieces : 2 + n_pieces + n_z]
    keys_ref, vals_ref, mixed_ref = rest[2 + n_pieces + n_z :]
    row = 0
    for piece in pieces:
        rows = piece.shape[1]
        keys_ref[row : row + rows] = piece[0]
        vals_ref[row : row + rows, :HD] = piece[1]
        row += rows
    vals_ref[:, HD:] = jnp.ones((row, HD), BF16)
    factor = HD ** (-0.5) * 1.4426950408889634
    part = q_own.shape[2]
    heads = q_own.shape[-1] // HD
    n_chunks = max(1, row // KEY_CHUNK)
    cut = row // n_chunks
    tile = CORES * heads * part // 2

    def one(n, carry):
        block = lax.rem(z_ref[0] + n, n_z)
        at = pl.multiple_of(block * part, 16)
        cosine, sine = cos_ref[pl.ds(at, part)], sin_ref[pl.ds(at, part)]
        queries = []
        for field in (q_own[block, core_ref[0]], q_other[block]):
            for head in range(heads):
                vec = field[:, head * HD : (head + 1) * HD].astype(F32)
                queries.append(norm_turn(vec, gain_ref[...], cosine, sine).astype(BF16))
        query = jnp.concatenate(queries, axis=0)
        tiles = [query[:tile], query[tile:]]
        score = lambda side, c: lax.dot_general(
            tiles[side], keys_ref[c * cut : (c + 1) * cut],
            (((1,), (1,)), ((), ())), preferred_element_type=F32,
        )
        work = [(c, side) for c in range(n_chunks) for side in range(2)]
        top, total = [None] * 2, [None] * 2
        scores = score(0, 0)
        for step, (c, side) in enumerate(work):
            after = score(work[step + 1][1], work[step + 1][0]) if step + 1 < len(work) else None
            here = jnp.max(scores, axis=1, keepdims=True)
            if c:
                here = jnp.maximum(top[side], here)
                shrink = jnp.exp2((top[side] - here) * factor)
            weights = jnp.exp2((scores - here) * factor).astype(BF16)
            part_sum = jnp.dot(
                weights, vals_ref[c * cut : (c + 1) * cut], preferred_element_type=F32
            )
            total[side] = total[side] * shrink + part_sum if c else part_sum
            top[side] = here
            scores = after
        mixed = None
        for side, weight in enumerate((w_own, w_other)):
            merged = (total[side][:, :HD] / total[side][:, HD:]).astype(BF16)
            merged = jnp.concatenate(
                [merged[h * part : (h + 1) * part] for h in range(heads)], axis=1
            )
            out = jnp.dot(merged, weight[...], preferred_element_type=F32)
            mixed = out if mixed is None else mixed + out
        mixed_ref[n] = mixed.astype(BF16)
        return carry

    lax.fori_loop(0, n_z, one, 0)
    for n, out_ref in enumerate(outs):
        out_ref[...] = mixed_ref[n]


def mix(core, z_index, queries, q_other, gain, cosine, sine, w_own, w_other, pieces, n_z):
    rows, width = cosine.shape[0], queries.shape[-1]
    part = rows // n_z
    d_model = w_own.shape[-1]
    length = sum(p.shape[1] for p in pieces)
    return pl.pallas_call(
        lambda *refs: mix_kernel(len(pieces), n_z, *refs),
        in_specs=[IN_SMEM] * 2 + [IN_VMEM] * (7 + len(pieces)),
        out_specs=[IN_VMEM] * n_z,
        out_shape=[jax.ShapeDtypeStruct((part, d_model), BF16)] * n_z,
        scratch_shapes=[
            pltpu.VMEM((length, HD), BF16),
            pltpu.VMEM((length, 2 * HD), BF16),
            pltpu.VMEM((n_z, part, d_model), BF16),
        ],
        compiler_params=pltpu.CompilerParams(vmem_limit_bytes=32 * MIB),
        name="mix",
    )(
        core, z_index, queries.reshape(n_z, CORES, part, width), q_other, gain, cosine, sine,
        w_own, w_other, *pieces,
    )


def dispatch_kernel(core_ref, tokens_ref, gain_ref, slots_ref, *out_refs):
    rows, d_model = slots_ref.shape[-1], tokens_ref.shape[-1]
    field = tokens_ref[...].reshape(rows, d_model).astype(F32)
    mean = jnp.mean(field * field, axis=-1, keepdims=True)
    normed = (field * lax.rsqrt(mean + EPS) * gain_ref[...]).astype(BF16)
    for chunk, out_ref in enumerate(out_refs):
        n_slots = out_ref.shape[0]
        slot = lax.broadcasted_iota(jnp.int32, (n_slots, rows), 0) + chunk * n_slots
        hot = slot == slots_ref[0:1]
        for k in range(1, TOPK):
            hot = hot | (slot == slots_ref[k : k + 1])
        out_ref[...] = jnp.dot(
            hot.astype(F32).astype(BF16), normed, preferred_element_type=F32
        ).astype(BF16)


def dispatch(core, tokens, gain, slots, n_z, pieces):
    local_rows, d_model = tokens.shape
    part = local_rows // (n_z * CORES)
    n_slots = EXPERTS * n_z * CAP // pieces
    return pl.pallas_call(
        dispatch_kernel,
        grid_spec=pltpu.PrefetchScalarGridSpec(
            num_scalar_prefetch=1,
            grid=(1,),
            in_specs=[
                pl.BlockSpec((n_z, 1, part, d_model), lambda i, c: (0, c[0], 0, 0)),
                pl.BlockSpec((1, d_model), lambda i, c: (0, 0)),
                pl.BlockSpec(slots.shape, lambda i, c: (0, 0)),
            ],
            out_specs=[IN_VMEM] * pieces,
        ),
        out_shape=[jax.ShapeDtypeStruct((n_slots, d_model), BF16)] * pieces,
        compiler_params=pltpu.CompilerParams(vmem_limit_bytes=16 * MIB),
        name="dispatch",
    )(core, *in_hbm([tokens.reshape(n_z, CORES, part, d_model)]), gain, slots)


def expert_kernel(n_src, group, *refs):
    ins, (gate_ref, up_ref, down_ref) = refs[: 2 * n_src], refs[2 * n_src : 2 * n_src + 3]
    outs, acc_ref = refs[2 * n_src + 3 : -1], refs[-1]
    expert, step = pl.program_id(0), pl.program_id(1)
    last = pl.num_programs(1) - 1
    rows = ins[0].shape[1]
    for first in range(0, len(ins), group):
        field = jnp.concatenate([ref[expert] for ref in ins[first : first + group]], axis=0)
        gate = jnp.dot(field, gate_ref[0], preferred_element_type=F32)
        up = jnp.dot(field, up_ref[0], preferred_element_type=F32)
        hidden = (gate / (1.0 + jnp.exp(-gate)) * up).astype(BF16)
        result = jnp.dot(hidden, down_ref[0], preferred_element_type=F32)
        here = slice(first * rows, (first + group) * rows)

        def finish(whole):
            for n, ref in enumerate(outs[first : first + group]):
                ref[expert] = whole[n * rows : (n + 1) * rows].astype(BF16)

        if acc_ref.shape[0] < len(ins) * rows:
            finish(result)
            continue

        @pl.when(step == 0)
        def _():
            acc_ref[here] = result

        @pl.when((step > 0) & (step < last))
        def _():
            acc_ref[here] += result

        @pl.when(step == last)
        def _():
            finish(acc_ref[here] + result)


def experts(own, other, gate_weight, up_weight, down_weight, first):
    pieces = [*own, *other]
    per, rows, d_model = pieces[0].shape
    width = gate_weight.shape[-1]
    cut = min(width, 256)
    steps = width // cut
    group = min(len(pieces), max(1, 256 // rows))
    outs = pl.pallas_call(
        lambda *refs: expert_kernel(len(own), group, *refs),
        grid=(per, steps),
        in_specs=[IN_VMEM] * len(pieces)
        + [
            pl.BlockSpec((1, d_model, cut), lambda e, s: (e + first, 0, s)),
            pl.BlockSpec((1, d_model, cut), lambda e, s: (e + first, 0, s)),
            pl.BlockSpec((1, cut, d_model), lambda e, s: (e + first, s, 0)),
        ],
        out_specs=[IN_VMEM] * len(pieces),
        out_shape=[jax.ShapeDtypeStruct((per, rows, d_model), BF16)] * len(pieces),
        scratch_shapes=[pltpu.VMEM((len(pieces) * rows if steps > 1 else 8, d_model), F32)],
        compiler_params=pltpu.CompilerParams(vmem_limit_bytes=32 * MIB),
        name="experts",
    )(*pieces, *in_hbm([gate_weight, up_weight, down_weight]))
    return outs[: len(own)], outs[len(own) :]


def combine_kernel(n_back, z_ref, slots_ref, shares_ref, *rest):
    back_refs, out_refs, total_ref = rest[:n_back], rest[n_back:-1], rest[-1]
    rows = slots_ref.shape[0]
    back = jnp.concatenate([ref[...] for ref in back_refs], axis=0)
    slot = lax.broadcasted_iota(jnp.int32, (rows, back.shape[0]), 1)
    matrix = jnp.zeros(slot.shape, F32)
    for k in range(TOPK):
        share = shares_ref[:, k : k + 1]
        matrix = matrix + jnp.where(slot == slots_ref[:, k : k + 1], share, 0.0)
    high = matrix.astype(BF16)
    low = (matrix - high.astype(F32)).astype(BF16)
    both = jnp.dot(jnp.concatenate([high, low], axis=0), back, preferred_element_type=F32)
    total_ref[...] = (both[:rows] + both[rows:]).reshape(total_ref.shape)
    n_z = len(out_refs)
    for n, out_ref in enumerate(out_refs):
        out_ref[...] = total_ref[lax.rem(z_ref[0] + n, n_z)].astype(BF16)


def combine(z_index, slots, shares, backs, n_z):
    rows, d_model = slots.shape[0], backs[0].shape[-1]
    return pl.pallas_call(
        lambda *refs: combine_kernel(len(backs), *refs),
        in_specs=[IN_SMEM] + [IN_VMEM] * (2 + len(backs)),
        out_specs=[IN_VMEM] * n_z,
        out_shape=[jax.ShapeDtypeStruct((rows // n_z, d_model), BF16)] * n_z,
        scratch_shapes=[pltpu.VMEM((n_z, rows // n_z, d_model), F32)],
        compiler_params=pltpu.CompilerParams(vmem_limit_bytes=24 * MIB),
        name="combine",
    )(z_index, slots, shares, *backs)


def shift(a, axis, step):
    n = lax.axis_size(axis)
    return lax.ppermute(a, axis, [(i, (i + step) % n) for i in range(n)])


def swap_cores(a):
    return lax.ppermute(a, "core", [(i, CORES - 1 - i) for i in range(CORES)])


def on_device(
    queries,
    keys,
    values,
    query_gain,
    key_gain,
    out_weight,
    tokens_b,
    norm_gain,
    routes,
    route_weight,
    gate_weight,
    up_weight,
    down_weight,
):
    n_ep, n_z = lax.axis_size("ep"), lax.axis_size("z")
    core, z_index = lax.axis_index("core"), lax.axis_index("z")
    core_arg = core.reshape(1).astype(jnp.int32)
    z_arg = z_index.reshape(1).astype(jnp.int32)
    n_rows, width = queries.shape
    d_model = tokens_b.shape[-1]
    heads = width // HD
    n_heads = heads * n_z * CORES

    part = n_rows // (n_z * CORES)
    offsets = (
        jnp.arange(n_z, dtype=jnp.int32)[:, None] * (CORES * part)
        + core * part
        + jnp.arange(part, dtype=jnp.int32)[None, :]
    ).reshape(-1)
    cosine, sine = rope_tables(lax.axis_index("ep") * n_rows + offsets)
    kv_head = ((z_index * CORES + core) * heads // (n_heads // KVH)).reshape(1).astype(jnp.int32)
    own_kv, q_send = prepare(
        core_arg, kv_head, keys, values, queries, key_gain[None], cosine, sine, n_z
    )
    pieces = [own_kv]
    for step in range(1, n_ep):
        pieces.append(shift(own_kv, "ep", step))
    pieces = pieces + [swap_cores(p) for p in pieces]

    q_other = swap_cores(q_send)
    w_other = swap_cores(out_weight)

    n_local = gate_weight.shape[0]
    chunks = 2 if n_local % 2 == 0 else 1
    per = n_local // chunks
    block_rows = tokens_b.shape[0] // (n_z * CORES)
    picks = block_rows * TOPK
    own_block = lambda a: lax.dynamic_index_in_dim(
        a.reshape(n_z, CORES, block_rows, TOPK), core, 1, keepdims=False
    )
    own_routes = own_block(routes)
    assigned = own_routes.reshape(n_z, picks)
    earlier = jnp.arange(picks)[:, None] > jnp.arange(picks)[None, :]
    same = (assigned[:, :, None] == assigned[:, None, :]) & earlier[None]
    rank = jnp.sum(same.astype(jnp.int32), axis=-1)
    block = jnp.arange(n_z, dtype=jnp.int32)[:, None]
    local = assigned % n_local
    ahead = lax.rem(assigned // n_local + n_ep - lax.axis_index("ep"), n_ep)
    place = ((local // per) * n_ep + ahead) * per + local % per
    slots = ((place * n_z + block) * CAP + rank).reshape(n_z * block_rows, TOPK)
    own_weight = own_block(route_weight).reshape(n_z * block_rows, TOPK)
    shares = own_weight / jnp.sum(own_weight, axis=-1, keepdims=True)
    slots, shares = lax.optimization_barrier((slots, shares))

    outgoing = dispatch(core_arg, tokens_b, norm_gain[None], slots.T, n_z, chunks * n_ep)
    arrived = []
    for chunk in range(chunks):
        here = []
        for step in range(n_ep):
            piece = outgoing[chunk * n_ep + step].reshape(per, n_z * CAP, d_model)
            here.append(shift(piece, "ep", step) if step else piece)
        arrived.append((here, [swap_cores(p) for p in here]))

    mixed = mix(
        core_arg, z_arg, queries, q_other, query_gain[None], cosine, sine, out_weight, w_other,
        pieces, n_z,
    )
    gathered = [mixed[0]]
    for step in range(1, n_z):
        gathered.append(shift(mixed[step], "z", step))
    mixed_out = add(*gathered)

    backs = []
    for chunk in range(chunks):
        keep, send = experts(
            *arrived[chunk], gate_weight, up_weight, down_weight, chunk * per
        )
        for step in range(n_ep):
            there = swap_cores(send[step])
            result = add(keep[step], there)
            result = shift(result, "ep", n_ep - step) if step else result
            backs.append(result.reshape(-1, d_model))
    rows = combine(z_arg, slots, shares, backs, n_z)
    gathered = [rows[0]]
    for step in range(1, n_z):
        gathered.append(shift(rows[step], "z", step))
    expert_out = add(*gathered)
    return (mixed_out, expert_out)


def solution(mesh):
    n_ep, n_tp = mesh.shape["ep"], mesh.shape["tp"]
    fine = Mesh(mesh.devices.reshape(n_ep, n_tp // CORES, CORES), ("ep", "z", "core"))
    tp = ("z", "core")
    placed = (
        P("ep", tp),
        P("ep", None),
        P("ep", None),
        P(),
        P(),
        P(tp, None),
        P("ep", None),
        P(),
        P("ep", None),
        P("ep", None),
        P("ep", None, tp),
        P("ep", None, tp),
        P("ep", tp, None),
    )

    return jax.shard_map(
        on_device,
        mesh=fine,
        in_specs=placed,
        out_specs=(P(("ep", "z", "core"), None), P(("ep", "z", "core"), None)),
        check_vma=False,
    )
```

```python
import jax
import jax.numpy as jnp
from jax import lax
from jax.experimental import pallas as pl
from jax.experimental.pallas import tpu as pltpu
from jax.sharding import Mesh, PartitionSpec as P


HD = 128
KVH = 4
EXPERTS = 16
TOPK = 2
GRID_W = 64
CAP = 8
EPS = 1e-06
THETA = 10000.0
CORES = 2
IN_VMEM = pl.BlockSpec(memory_space=pltpu.VMEM)
IN_SMEM = pl.BlockSpec(memory_space=pltpu.SMEM)
KEY_CHUNK = 1024
MIB = 1024 * 1024

F32 = jnp.float32
BF16 = jnp.bfloat16


def in_hbm(arrays):
    return [pltpu.with_memory_space_constraint(a, pltpu.HBM) for a in arrays]


def rope_tables(positions):
    n_freq = HD // 4
    row_pos = (positions // GRID_W).astype(F32)[:, None]
    col_pos = (positions % GRID_W).astype(F32)[:, None]
    lane = jnp.arange(HD, dtype=jnp.int32)
    inverse = THETA ** (-(lane % n_freq).astype(F32) / n_freq)
    angle = jnp.where(lane < HD // 2, row_pos, col_pos) * inverse
    sign = jnp.where((lane // n_freq) % 2 == 0, -1.0, 1.0).astype(F32)
    return jnp.cos(angle), jnp.sin(angle) * sign


def norm_turn(field, gain, cosine, sine):
    quarter = HD // 4
    mean = jnp.mean(field * field, axis=-1, keepdims=True)
    field = field * lax.rsqrt(mean + EPS) * gain
    lane = lax.broadcasted_iota(jnp.int32, field.shape, 1)
    partner = jnp.where(
        (lane // quarter) % 2 == 0,
        pltpu.roll(field, HD - quarter, 1),
        pltpu.roll(field, quarter, 1),
    )
    return field * cosine + partner * sine


def prepare_kernel(
    core_ref, head_ref, keys_ref, values_ref, q_ref, own_ref, gain_ref, cos_ref, sin_ref,
    kv_ref, send_ref, keep_ref,
):
    rows = cos_ref.shape[0]
    field = keys_ref[...].reshape(rows, HD).astype(F32)
    kv_ref[0] = norm_turn(field, gain_ref[...], cos_ref[...], sin_ref[...]).astype(BF16)
    kv_ref[1] = values_ref[...].reshape(rows, HD)
    send_ref[...] = q_ref[...].reshape(send_ref.shape)
    keep_ref[...] = own_ref[...].reshape(keep_ref.shape)


def prepare(core, head, keys, values, queries, gain, cosine, sine, n_z):
    rows, width = cosine.shape[0], queries.shape[-1]
    part = rows // n_z
    view = lambda a: a.reshape(n_z, CORES, part, a.shape[-1])
    picked = pl.BlockSpec((n_z, 1, part, HD), lambda i, c, h: (0, c[0], 0, h[0]))
    whole = lambda shape: pl.BlockSpec(shape, lambda i, c, h: (0,) * len(shape))
    return pl.pallas_call(
        prepare_kernel,
        grid_spec=pltpu.PrefetchScalarGridSpec(
            num_scalar_prefetch=2,
            grid=(1,),
            in_specs=[
                picked,
                picked,
                pl.BlockSpec((n_z, 1, part, width), lambda i, c, h: (0, 1 - c[0], 0, 0)),
                pl.BlockSpec((n_z, 1, part, width), lambda i, c, h: (0, c[0], 0, 0)),
                whole((1, HD)),
                whole((rows, HD)),
                whole((rows, HD)),
            ],
            out_specs=[IN_VMEM] * 3,
        ),
        out_shape=[
            jax.ShapeDtypeStruct((2, rows, HD), BF16),
            jax.ShapeDtypeStruct((n_z, part, width), BF16),
            jax.ShapeDtypeStruct((n_z, part, width), BF16),
        ],
        compiler_params=pltpu.CompilerParams(vmem_limit_bytes=8 * MIB),
        name="prepare",
    )(
        core, head, *in_hbm([view(keys), view(values), view(queries), view(queries), gain]),
        cosine, sine,
    )


def add_kernel(*refs):
    total = refs[0][...].astype(F32)
    for ref in refs[1:-1]:
        total = total + ref[...].astype(F32)
    refs[-1][...] = total.astype(BF16)


def add(*arrays):
    return pl.pallas_call(
        add_kernel,
        in_specs=[IN_VMEM] * len(arrays),
        out_specs=IN_VMEM,
        out_shape=jax.ShapeDtypeStruct(arrays[0].shape, BF16),
        compiler_params=pltpu.CompilerParams(vmem_limit_bytes=8 * MIB),
        name="add",
    )(*arrays)


def mix_kernel(n_pieces, n_z, z_ref, q_own, q_other, gain_hbm, cos_ref, sin_ref, w_other, *rest):
    sources = [gain_hbm, rest[0], *[w.at[pl.ds(0, o.shape[0])] for w, o in zip(
        rest[1:4], rest[4 + n_pieces + n_z : 7 + n_pieces + n_z])]]
    pieces = rest[4 : 4 + n_pieces]
    outs = rest[4 + n_pieces : 4 + n_pieces + n_z]
    loaded = rest[4 + n_pieces + n_z : 7 + n_pieces + n_z]
    keys_ref, vals_ref, mixed_ref, w_own, gain_ref, sems = rest[7 + n_pieces + n_z :]
    copies = [
        pltpu.make_async_copy(source, target, sems.at[n])
        for n, (source, target) in enumerate(zip(sources, (gain_ref, w_own, *loaded)))
    ]
    for copy in copies:
        copy.start()
    row = 0
    for piece in pieces:
        rows = piece.shape[1]
        keys_ref[row : row + rows] = piece[0]
        vals_ref[row : row + rows, :HD] = piece[1]
        row += rows
    vals_ref[:, HD:] = jnp.ones((row, HD), BF16)
    factor = HD ** (-0.5) * 1.4426950408889634
    part = q_own.shape[1]
    heads = q_own.shape[-1] // HD
    n_chunks = max(1, row // KEY_CHUNK)
    cut = row // n_chunks
    tile = CORES * heads * part // 2

    copies[0].wait()
    copies[1].wait()

    def one(n, carry):
        block = lax.rem(z_ref[0] + n, n_z)
        at = pl.multiple_of(block * part, 16)
        cosine, sine = cos_ref[pl.ds(at, part)], sin_ref[pl.ds(at, part)]
        queries = []
        for field in (q_own[block], q_other[block]):
            for head in range(heads):
                vec = field[:, head * HD : (head + 1) * HD].astype(F32)
                queries.append(norm_turn(vec, gain_ref[...], cosine, sine).astype(BF16))
        query = jnp.concatenate(queries, axis=0)
        tiles = [query[:tile], query[tile:]]
        score = lambda side, c: lax.dot_general(
            tiles[side], keys_ref[c * cut : (c + 1) * cut],
            (((1,), (1,)), ((), ())), preferred_element_type=F32,
        )
        work = [(c, side) for c in range(n_chunks) for side in range(2)]
        top, total = [None] * 2, [None] * 2
        scores = score(0, 0)
        for step, (c, side) in enumerate(work):
            after = score(work[step + 1][1], work[step + 1][0]) if step + 1 < len(work) else None
            here = jnp.max(scores, axis=1, keepdims=True)
            if c:
                here = jnp.maximum(top[side], here)
                shrink = jnp.exp2((top[side] - here) * factor)
            weights = jnp.exp2((scores - here) * factor).astype(BF16)
            part_sum = jnp.dot(
                weights, vals_ref[c * cut : (c + 1) * cut], preferred_element_type=F32
            )
            total[side] = total[side] * shrink + part_sum if c else part_sum
            top[side] = here
            scores = after
        mixed = None
        for side, weight in enumerate((w_own, w_other)):
            merged = (total[side][:, :HD] / total[side][:, HD:]).astype(BF16)
            merged = jnp.concatenate(
                [merged[h * part : (h + 1) * part] for h in range(heads)], axis=1
            )
            out = jnp.dot(merged, weight[...], preferred_element_type=F32)
            mixed = out if mixed is None else mixed + out
        mixed_ref[n] = mixed.astype(BF16)
        return carry

    lax.fori_loop(0, n_z, one, 0)
    for n, out_ref in enumerate(outs):
        out_ref[...] = mixed_ref[n]
    for copy in copies[2:]:
        copy.wait()


def mix(z_index, q_own, q_other, gain, cosine, sine, w_own, w_other, weights, per, pieces):
    n_z, part, _ = q_own.shape
    d_model = w_own.shape[-1]
    length = sum(p.shape[1] for p in pieces)
    any_space = pl.BlockSpec(memory_space=pl.ANY)
    outs = pl.pallas_call(
        lambda *refs: mix_kernel(len(pieces), n_z, *refs),
        in_specs=[IN_SMEM, IN_VMEM, IN_VMEM, any_space, IN_VMEM, IN_VMEM, IN_VMEM]
        + [any_space] * 4
        + [IN_VMEM] * len(pieces),
        out_specs=[IN_VMEM] * (n_z + 3),
        out_shape=[jax.ShapeDtypeStruct((part, d_model), BF16)] * n_z
        + [jax.ShapeDtypeStruct((per, *w.shape[1:]), BF16) for w in weights],
        scratch_shapes=[
            pltpu.VMEM((length, HD), BF16),
            pltpu.VMEM((length, 2 * HD), BF16),
            pltpu.VMEM((n_z, part, d_model), BF16),
            pltpu.VMEM(w_own.shape, BF16),
            pltpu.VMEM(gain.shape, F32),
            pltpu.SemaphoreType.DMA((5,)),
        ],
        compiler_params=pltpu.CompilerParams(vmem_limit_bytes=20 * MIB),
        name="mix",
    )(
        z_index, q_own, q_other, *in_hbm([gain]), cosine, sine, w_other,
        *in_hbm([w_own, *weights]), *pieces,
    )
    return outs[:n_z], outs[n_z:]


def block_of(index, block, count):
    found = jnp.zeros_like(index)
    for n in range(1, count):
        found = found + (index >= n * block).astype(jnp.int32)
    return found


def dispatch_kernel(
    n_ep, n_local, core_ref, ep_ref, tokens_ref, gain_ref, routes_ref, weight_ref, *rest
):
    out_refs, cols_ref = rest[:n_ep], rest[n_ep]
    n_z, _, block, d_model = tokens_ref.shape
    rows, local_rows = n_z * block, routes_ref.shape[1]
    iota = lambda shape, dim: lax.broadcasted_iota(jnp.int32, shape, dim)
    exact = dict(preferred_element_type=F32, precision=lax.Precision.HIGHEST)

    lane = iota((local_rows, rows), 1)
    lane_block = block_of(lane, block, n_z)
    source = lane + (lane_block * (CORES - 1) + core_ref[0]) * block
    select = (iota((local_rows, rows), 0) == source).astype(F32)
    chosen = jnp.dot(routes_ref[...].astype(F32), select, **exact)
    chosen = (chosen + 0.5).astype(jnp.int32)
    weight = jnp.dot(weight_ref[...], select, **exact)

    shape = (EXPERTS, rows)
    expert = iota(shape, 0)
    hot = [expert == chosen[k : k + 1] for k in range(TOPK)]
    either = hot[0]
    for one in hot[1:]:
        either = either | one
    square = (rows, rows)
    above, across = iota(square, 0), iota(square, 1)
    first = block_of(across, block, n_z) * block
    earlier = ((above < across) & (above >= first)).astype(F32).astype(BF16)
    count = jnp.dot(either.astype(F32).astype(BF16), earlier, preferred_element_type=F32)
    owner = block_of(expert, n_local, n_ep)
    ahead = owner - ep_ref[0]
    ahead = jnp.where(ahead < 0, ahead + n_ep, ahead)
    place = (ahead * n_local + expert - owner * n_local) * (n_z * CAP)
    place = place + block_of(iota(shape, 1), block, n_z) * CAP + (count + 0.5).astype(jnp.int32)
    slots = [jnp.sum(jnp.where(h, place, 0), axis=0, keepdims=True) for h in hot]

    total = jnp.sum(weight, axis=0, keepdims=True)
    table = [s.astype(F32) for s in slots] + [weight[k : k + 1] / total for k in range(TOPK)]
    lines = iota((8, rows), 0)
    stacked = jnp.zeros((8, rows), F32)
    for n, line in enumerate(table):
        stacked = jnp.where(lines == n, line, stacked)
    same = (above == across).astype(F32)
    cols_ref[...] = lax.dot_general(same, stacked, (((1,), (1,)), ((), ())), **exact)

    field = tokens_ref[...].reshape(rows, d_model).astype(F32)
    mean = jnp.mean(field * field, axis=-1, keepdims=True)
    normed = (field * lax.rsqrt(mean + EPS) * gain_ref[...]).astype(BF16)
    n_slots = out_refs[0].shape[0]
    for piece, out_ref in enumerate(out_refs):
        slot = iota((n_slots, rows), 0) + piece * n_slots
        picked = slot == slots[0]
        for one in slots[1:]:
            picked = picked | (slot == one)
        picked = picked.astype(F32).astype(BF16)
        out_ref[...] = jnp.dot(picked, normed, preferred_element_type=F32).astype(BF16)


def dispatch(core, ep, tokens, gain, routes, weight, n_z, n_ep, n_local):
    local_rows, d_model = tokens.shape
    block = local_rows // (n_z * CORES)
    n_slots = n_local * n_z * CAP
    whole = lambda a: pl.BlockSpec(a.shape, lambda i, c, e: (0,) * a.ndim)
    outs = pl.pallas_call(
        lambda *refs: dispatch_kernel(n_ep, n_local, *refs),
        grid_spec=pltpu.PrefetchScalarGridSpec(
            num_scalar_prefetch=2,
            grid=(1,),
            in_specs=[
                pl.BlockSpec((n_z, 1, block, d_model), lambda i, c, e: (0, c[0], 0, 0)),
                whole(gain),
                whole(routes),
                whole(weight),
            ],
            out_specs=[IN_VMEM] * (n_ep + 1),
        ),
        out_shape=[jax.ShapeDtypeStruct((n_slots, d_model), BF16)] * n_ep
        + [jax.ShapeDtypeStruct((n_z * block, 8), F32)],
        compiler_params=pltpu.CompilerParams(vmem_limit_bytes=16 * MIB),
        name="dispatch",
    )(core, ep, *in_hbm([tokens.reshape(n_z, CORES, block, d_model), gain]), routes, weight)
    return outs[:n_ep], outs[n_ep]


def expert_kernel(n_in, group, first, n_next, *refs):
    ins, (gate_ref, up_ref, down_ref) = refs[:n_in], refs[n_in : n_in + 3]
    sources, outs = refs[n_in + 3 : n_in + 3 + n_next], refs[n_in + 3 + n_next : 2 * n_in + 3 + n_next]
    per, rows, _ = outs[0].shape
    copies = []
    if n_next:
        targets, sems = refs[2 * n_in + 3 + n_next : -1], refs[-1]
        for n, (source, target) in enumerate(zip(sources, targets)):
            part = source.at[pl.ds(first + per, per)]
            copies.append(pltpu.make_async_copy(part, target, sems.at[n]))
    for copy in copies:
        copy.start()
    for expert in range(per):
        for start in range(0, len(ins), group):
            field = [ref[first + expert] for ref in ins[start : start + group]]
            field = jnp.concatenate(field, axis=0)
            gate = jnp.dot(field, gate_ref[expert], preferred_element_type=F32)
            up = jnp.dot(field, up_ref[expert], preferred_element_type=F32)
            hidden = (gate / (1.0 + jnp.exp(-gate)) * up).astype(BF16)
            result = jnp.dot(hidden, down_ref[expert], preferred_element_type=F32)
            for n, ref in enumerate(outs[start : start + group]):
                ref[expert] = result[n * rows : (n + 1) * rows].astype(BF16)
    for copy in copies:
        copy.wait()


def experts(own, other, weights, first, all_weights):
    pieces = [*own, *other]
    _, rows, d_model = pieces[0].shape
    per = weights[0].shape[0]
    more = in_hbm(all_weights) if first + per < all_weights[0].shape[0] else []
    group = min(len(pieces), max(1, 256 // rows))
    outs = pl.pallas_call(
        lambda *refs: expert_kernel(len(pieces), group, first, len(more), *refs),
        in_specs=[IN_VMEM] * (len(pieces) + 3) + [pl.BlockSpec(memory_space=pl.ANY)] * len(more),
        out_specs=[IN_VMEM] * (len(pieces) + len(more)),
        out_shape=[jax.ShapeDtypeStruct((per, rows, d_model), BF16)] * len(pieces)
        + [jax.ShapeDtypeStruct((per, *w.shape[1:]), BF16) for w in more],
        scratch_shapes=[pltpu.SemaphoreType.DMA((len(more),))] if more else [],
        compiler_params=pltpu.CompilerParams(vmem_limit_bytes=16 * MIB),
        name="experts",
    )(*pieces, *weights, *more)
    return outs[: len(own)], outs[len(own) : len(pieces)], outs[len(pieces) :]


def combine_kernel(n_back, z_ref, cols_ref, *rest):
    back_refs, out_refs, total_ref = rest[:n_back], rest[n_back:-1], rest[-1]
    rows = cols_ref.shape[0]
    back = jnp.concatenate([ref[...] for ref in back_refs], axis=0)
    slot = lax.broadcasted_iota(jnp.int32, (rows, back.shape[0]), 1)
    matrix = jnp.zeros(slot.shape, F32)
    for k in range(TOPK):
        own = (cols_ref[:, k : k + 1] + 0.5).astype(jnp.int32)
        share = cols_ref[:, TOPK + k : TOPK + k + 1]
        matrix = matrix + jnp.where(slot == own, share, 0.0)
    high = matrix.astype(BF16)
    low = (matrix - high.astype(F32)).astype(BF16)
    both = jnp.dot(jnp.concatenate([high, low], axis=0), back, preferred_element_type=F32)
    total_ref[...] = (both[:rows] + both[rows:]).reshape(total_ref.shape)
    n_z = len(out_refs)
    for n, out_ref in enumerate(out_refs):
        out_ref[...] = total_ref[lax.rem(z_ref[0] + n, n_z)].astype(BF16)


def combine(z_index, cols, backs, n_z):
    rows, d_model = cols.shape[0], backs[0].shape[-1]
    return pl.pallas_call(
        lambda *refs: combine_kernel(len(backs), *refs),
        in_specs=[IN_SMEM] + [IN_VMEM] * (1 + len(backs)),
        out_specs=[IN_VMEM] * n_z,
        out_shape=[jax.ShapeDtypeStruct((rows // n_z, d_model), BF16)] * n_z,
        scratch_shapes=[pltpu.VMEM((n_z, rows // n_z, d_model), F32)],
        compiler_params=pltpu.CompilerParams(vmem_limit_bytes=24 * MIB),
        name="combine",
    )(z_index, cols, *backs)


def shift(a, axis, step):
    n = lax.axis_size(axis)
    return lax.ppermute(a, axis, [(i, (i + step) % n) for i in range(n)])


def swap_cores(a):
    return lax.ppermute(a, "core", [(i, CORES - 1 - i) for i in range(CORES)])


def on_device(
    queries,
    keys,
    values,
    query_gain,
    key_gain,
    out_weight,
    tokens_b,
    norm_gain,
    routes,
    route_weight,
    gate_weight,
    up_weight,
    down_weight,
):
    n_ep, n_z = lax.axis_size("ep"), lax.axis_size("z")
    core, z_index = lax.axis_index("core"), lax.axis_index("z")
    core_arg = core.reshape(1).astype(jnp.int32)
    z_arg = z_index.reshape(1).astype(jnp.int32)
    n_rows, width = queries.shape
    d_model = tokens_b.shape[-1]
    heads = width // HD
    n_heads = heads * n_z * CORES

    part = n_rows // (n_z * CORES)
    offsets = (
        jnp.arange(n_z, dtype=jnp.int32)[:, None] * (CORES * part)
        + core * part
        + jnp.arange(part, dtype=jnp.int32)[None, :]
    ).reshape(-1)
    cosine, sine = rope_tables(lax.axis_index("ep") * n_rows + offsets)
    kv_head = ((z_index * CORES + core) * heads // (n_heads // KVH)).reshape(1).astype(jnp.int32)
    own_kv, q_send, q_own = prepare(
        core_arg, kv_head, keys, values, queries, key_gain[None], cosine, sine, n_z
    )
    pieces = [own_kv]
    for step in range(1, n_ep):
        pieces.append(shift(own_kv, "ep", step))
    pieces = pieces + [swap_cores(p) for p in pieces]

    q_other = swap_cores(q_send)
    w_other = swap_cores(out_weight)

    n_local = gate_weight.shape[0]
    chunks = 2 if n_local % 2 == 0 else 1
    per = n_local // chunks
    ep_arg = lax.axis_index("ep").reshape(1).astype(jnp.int32)
    outgoing, cols = dispatch(
        core_arg, ep_arg, tokens_b, norm_gain[None], routes.T, route_weight.T, n_z, n_ep, n_local
    )
    here = []
    for step in range(n_ep):
        piece = outgoing[step].reshape(n_local, n_z * CAP, d_model)
        here.append(shift(piece, "ep", step) if step else piece)
    there = [swap_cores(p) for p in here]

    all_weights = [gate_weight, up_weight, down_weight]
    mixed, weights = mix(
        z_arg, q_own, q_other, query_gain[None], cosine, sine, out_weight, w_other,
        all_weights, per, pieces,
    )
    gathered = [mixed[0]]
    for step in range(1, n_z):
        gathered.append(shift(mixed[step], "z", step))
    mixed_out = add(*gathered)

    backs = [[] for _ in range(n_ep)]
    for chunk in range(chunks):
        keep, send, weights = experts(here, there, weights, chunk * per, all_weights)
        for step in range(n_ep):
            result = add(keep[step], swap_cores(send[step]))
            result = shift(result, "ep", n_ep - step) if step else result
            backs[step].append(result.reshape(-1, d_model))
    rows = combine(z_arg, cols, [b for step in backs for b in step], n_z)
    gathered = [rows[0]]
    for step in range(1, n_z):
        gathered.append(shift(rows[step], "z", step))
    expert_out = add(*gathered)
    return (mixed_out, expert_out)


def solution(mesh):
    n_ep, n_tp = mesh.shape["ep"], mesh.shape["tp"]
    fine = Mesh(mesh.devices.reshape(n_ep, n_tp // CORES, CORES), ("ep", "z", "core"))
    tp = ("z", "core")
    placed = (
        P("ep", tp),
        P("ep", None),
        P("ep", None),
        P(),
        P(),
        P(tp, None),
        P("ep", None),
        P(),
        P("ep", None),
        P("ep", None),
        P("ep", None, tp),
        P("ep", None, tp),
        P("ep", tp, None),
    )

    return jax.shard_map(
        on_device,
        mesh=fine,
        in_specs=placed,
        out_specs=(P(("ep", "z", "core"), None), P(("ep", "z", "core"), None)),
        check_vma=False,
    )
```

```python
import jax
import jax.numpy as jnp
from jax import lax
from jax.experimental import pallas as pl
from jax.experimental.pallas import tpu as pltpu
from jax.sharding import Mesh, PartitionSpec as P


HD = 128
KVH = 4
EXPERTS = 16
TOPK = 2
GRID_W = 64
CAP = 8
EPS = 1e-06
THETA = 10000.0
CORES = 2
IN_VMEM = pl.BlockSpec(memory_space=pltpu.VMEM)
IN_SMEM = pl.BlockSpec(memory_space=pltpu.SMEM)
SPLIT = 2
KEY_CHUNK = 1024
MIB = 1024 * 1024

F32 = jnp.float32
BF16 = jnp.bfloat16


def in_hbm(arrays):
    return [pltpu.with_memory_space_constraint(a, pltpu.HBM) for a in arrays]


def rope_tables(positions):
    n_freq = HD // 4
    row_pos = (positions // GRID_W).astype(F32)[:, None]
    col_pos = (positions % GRID_W).astype(F32)[:, None]
    lane = jnp.arange(HD, dtype=jnp.int32)
    inverse = THETA ** (-(lane % n_freq).astype(F32) / n_freq)
    angle = jnp.where(lane < HD // 2, row_pos, col_pos) * inverse
    sign = jnp.where((lane // n_freq) % 2 == 0, -1.0, 1.0).astype(F32)
    return jnp.cos(angle), jnp.sin(angle) * sign


def norm_turn(field, gain, cosine, sine):
    quarter = HD // 4
    mean = jnp.mean(field * field, axis=-1, keepdims=True)
    field = field * lax.rsqrt(mean + EPS) * gain
    lane = lax.broadcasted_iota(jnp.int32, field.shape, 1)
    partner = jnp.where(
        (lane // quarter) % 2 == 0,
        pltpu.roll(field, HD - quarter, 1),
        pltpu.roll(field, quarter, 1),
    )
    return field * cosine + partner * sine


def prepare_kernel(
    core_ref, head_ref, keys_ref, values_ref, q_ref, own_ref, gain_ref, cos_ref, sin_ref,
    kv_ref, send_ref, keep_ref,
):
    rows = cos_ref.shape[0]
    field = keys_ref[...].reshape(rows, HD).astype(F32)
    kv_ref[0] = norm_turn(field, gain_ref[...], cos_ref[...], sin_ref[...]).astype(BF16)
    kv_ref[1] = values_ref[...].reshape(rows, HD)
    send_ref[...] = q_ref[...].reshape(send_ref.shape)
    keep_ref[...] = own_ref[...].reshape(keep_ref.shape)


def prepare(core, head, keys, values, queries, gain, cosine, sine, n_z):
    rows, width = cosine.shape[0], queries.shape[-1]
    part = rows // n_z
    view = lambda a: a.reshape(n_z, CORES, part, a.shape[-1])
    picked = pl.BlockSpec((n_z, 1, part, HD), lambda i, c, h: (0, c[0], 0, h[0]))
    whole = lambda shape: pl.BlockSpec(shape, lambda i, c, h: (0,) * len(shape))
    return pl.pallas_call(
        prepare_kernel,
        grid_spec=pltpu.PrefetchScalarGridSpec(
            num_scalar_prefetch=2,
            grid=(1,),
            in_specs=[
                picked,
                picked,
                pl.BlockSpec((n_z, 1, part, width), lambda i, c, h: (0, 1 - c[0], 0, 0)),
                pl.BlockSpec((n_z, 1, part, width), lambda i, c, h: (0, c[0], 0, 0)),
                whole((1, HD)),
                whole((rows, HD)),
                whole((rows, HD)),
            ],
            out_specs=[IN_VMEM] * 3,
        ),
        out_shape=[
            jax.ShapeDtypeStruct((2, rows, HD), BF16),
            jax.ShapeDtypeStruct((n_z, part, width), BF16),
            jax.ShapeDtypeStruct((n_z, part, width), BF16),
        ],
        compiler_params=pltpu.CompilerParams(vmem_limit_bytes=8 * MIB),
        name="prepare",
    )(
        core, head, *in_hbm([view(keys), view(values), view(queries), view(queries), gain]),
        cosine, sine,
    )


def add_kernel(*refs):
    total = refs[0][...].astype(F32)
    for ref in refs[1:-1]:
        total = total + ref[...].astype(F32)
    refs[-1][...] = total.astype(BF16)


def add(*arrays):
    return pl.pallas_call(
        add_kernel,
        in_specs=[IN_VMEM] * len(arrays),
        out_specs=IN_VMEM,
        out_shape=jax.ShapeDtypeStruct(arrays[0].shape, BF16),
        compiler_params=pltpu.CompilerParams(vmem_limit_bytes=8 * MIB),
        name="add",
    )(*arrays)


def weight_copies(sources, targets, first, sems, sem):
    copies = []
    for source, target in zip(sources, targets):
        per, rows, _ = target.shape
        cut = rows // SPLIT
        for expert in range(per):
            for n in range(SPLIT):
                part = pl.ds(n * cut, cut)
                copies.append(
                    pltpu.make_async_copy(
                        source.at[first + expert, part], target.at[expert, part], sems.at[sem]
                    )
                )
                sem += 1
    return copies


def mix_kernel(n_pieces, n_z, z_ref, q_own, q_other, gain_hbm, cos_ref, sin_ref, w_other, *rest):
    pieces = rest[4 : 4 + n_pieces]
    outs = rest[4 + n_pieces : 4 + n_pieces + n_z]
    loaded = rest[4 + n_pieces + n_z : 7 + n_pieces + n_z]
    keys_ref, vals_ref, mixed_ref, w_own, gain_ref, sems = rest[7 + n_pieces + n_z :]
    copies = [
        pltpu.make_async_copy(gain_hbm, gain_ref, sems.at[0]),
        pltpu.make_async_copy(rest[0], w_own, sems.at[1]),
        *weight_copies(rest[1:4], loaded, 0, sems, 2),
    ]
    for copy in copies:
        copy.start()
    row = 0
    for piece in pieces:
        rows = piece.shape[1]
        keys_ref[row : row + rows] = piece[0]
        vals_ref[row : row + rows, :HD] = piece[1]
        row += rows
    vals_ref[:, HD:] = jnp.ones((row, HD), BF16)
    factor = HD ** (-0.5) * 1.4426950408889634
    part = q_own.shape[1]
    heads = q_own.shape[-1] // HD
    n_chunks = max(1, row // KEY_CHUNK)
    cut = row // n_chunks
    tile = CORES * heads * part // 2

    copies[0].wait()
    copies[1].wait()

    def one(n, carry):
        block = peer(z_ref[0], n, n_z)
        at = pl.multiple_of(block * part, 16)
        cosine, sine = cos_ref[pl.ds(at, part)], sin_ref[pl.ds(at, part)]
        queries = []
        for field in (q_own[block], q_other[block]):
            for head in range(heads):
                vec = field[:, head * HD : (head + 1) * HD].astype(F32)
                queries.append(norm_turn(vec, gain_ref[...], cosine, sine).astype(BF16))
        query = jnp.concatenate(queries, axis=0)
        tiles = [query[:tile], query[tile:]]
        score = lambda side, c: lax.dot_general(
            tiles[side], keys_ref[c * cut : (c + 1) * cut],
            (((1,), (1,)), ((), ())), preferred_element_type=F32,
        )
        work = [(c, side) for c in range(n_chunks) for side in range(2)]
        top, total = [None] * 2, [None] * 2
        scores = score(0, 0)
        for step, (c, side) in enumerate(work):
            after = score(work[step + 1][1], work[step + 1][0]) if step + 1 < len(work) else None
            here = jnp.max(scores, axis=1, keepdims=True)
            if c:
                here = jnp.maximum(top[side], here)
                shrink = jnp.exp2((top[side] - here) * factor)
            weights = jnp.exp2((scores - here) * factor).astype(BF16)
            part_sum = jnp.dot(
                weights, vals_ref[c * cut : (c + 1) * cut], preferred_element_type=F32
            )
            total[side] = total[side] * shrink + part_sum if c else part_sum
            top[side] = here
            scores = after
        mixed = None
        for side, weight in enumerate((w_own, w_other)):
            merged = (total[side][:, :HD] / total[side][:, HD:]).astype(BF16)
            merged = jnp.concatenate(
                [merged[h * part : (h + 1) * part] for h in range(heads)], axis=1
            )
            out = jnp.dot(merged, weight[...], preferred_element_type=F32)
            mixed = out if mixed is None else mixed + out
        mixed_ref[n] = mixed.astype(BF16)
        return carry

    lax.fori_loop(0, n_z, one, 0)
    for n, out_ref in enumerate(outs):
        out_ref[...] = mixed_ref[n]
    for copy in copies[2:]:
        copy.wait()


def mix(z_index, q_own, q_other, gain, cosine, sine, w_own, w_other, weights, per, pieces):
    n_z, part, _ = q_own.shape
    d_model = w_own.shape[-1]
    length = sum(p.shape[1] for p in pieces)
    any_space = pl.BlockSpec(memory_space=pl.ANY)
    outs = pl.pallas_call(
        lambda *refs: mix_kernel(len(pieces), n_z, *refs),
        in_specs=[IN_SMEM, IN_VMEM, IN_VMEM, any_space, IN_VMEM, IN_VMEM, IN_VMEM]
        + [any_space] * 4
        + [IN_VMEM] * len(pieces),
        out_specs=[IN_VMEM] * (n_z + 3),
        out_shape=[jax.ShapeDtypeStruct((part, d_model), BF16)] * n_z
        + [jax.ShapeDtypeStruct((per, *w.shape[1:]), BF16) for w in weights],
        scratch_shapes=[
            pltpu.VMEM((length, HD), BF16),
            pltpu.VMEM((length, 2 * HD), BF16),
            pltpu.VMEM((n_z, part, d_model), BF16),
            pltpu.VMEM(w_own.shape, BF16),
            pltpu.VMEM(gain.shape, F32),
            pltpu.SemaphoreType.DMA((2 + 3 * per * SPLIT,)),
        ],
        compiler_params=pltpu.CompilerParams(vmem_limit_bytes=20 * MIB),
        name="mix",
    )(
        z_index, q_own, q_other, *in_hbm([gain]), cosine, sine, w_other,
        *in_hbm([w_own, *weights]), *pieces,
    )
    return outs[:n_z], outs[n_z:]


def block_of(index, block, count):
    found = jnp.zeros_like(index)
    for n in range(1, count):
        found = found + (index >= n * block).astype(jnp.int32)
    return found


def dispatch_kernel(
    n_ep, n_local, per, core_ref, ep_ref, tokens_ref, gain_ref, routes_ref, weight_ref, *rest
):
    out_refs, cols_ref = rest[:-1], rest[-1]
    n_z, _, block, d_model = tokens_ref.shape
    rows, local_rows = n_z * block, routes_ref.shape[1]
    iota = lambda shape, dim: lax.broadcasted_iota(jnp.int32, shape, dim)
    exact = dict(preferred_element_type=F32, precision=lax.Precision.HIGHEST)

    lane = iota((local_rows, rows), 1)
    lane_block = block_of(lane, block, n_z)
    source = lane + (lane_block * (CORES - 1) + core_ref[0]) * block
    select = (iota((local_rows, rows), 0) == source).astype(F32)
    chosen = jnp.dot(routes_ref[...].astype(F32), select, **exact)
    chosen = (chosen + 0.5).astype(jnp.int32)
    weight = jnp.dot(weight_ref[...], select, **exact)

    shape = (EXPERTS, rows)
    expert = iota(shape, 0)
    hot = [expert == chosen[k : k + 1] for k in range(TOPK)]
    either = hot[0]
    for one in hot[1:]:
        either = either | one
    square = (rows, rows)
    above, across = iota(square, 0), iota(square, 1)
    first = block_of(across, block, n_z) * block
    earlier = ((above < across) & (above >= first)).astype(F32).astype(BF16)
    count = jnp.dot(either.astype(F32).astype(BF16), earlier, preferred_element_type=F32)
    owner = block_of(expert, n_local, n_ep)
    if n_ep & (n_ep - 1) == 0:
        ahead = owner ^ ep_ref[0]
    else:
        ahead = owner - ep_ref[0]
        ahead = jnp.where(ahead < 0, ahead + n_ep, ahead)
    local = expert - owner * n_local
    turn = block_of(local, per, n_local // per)
    place = ((turn * n_ep + ahead) * per + local - turn * per) * (n_z * CAP)
    place = place + block_of(iota(shape, 1), block, n_z) * CAP + (count + 0.5).astype(jnp.int32)
    slots = [jnp.sum(jnp.where(h, place, 0), axis=0, keepdims=True) for h in hot]

    total = jnp.sum(weight, axis=0, keepdims=True)
    table = [s.astype(F32) for s in slots] + [weight[k : k + 1] / total for k in range(TOPK)]
    lines = iota((8, rows), 0)
    stacked = jnp.zeros((8, rows), F32)
    for n, line in enumerate(table):
        stacked = jnp.where(lines == n, line, stacked)
    same = (above == across).astype(F32)
    cols_ref[...] = lax.dot_general(same, stacked, (((1,), (1,)), ((), ())), **exact)

    field = tokens_ref[...].reshape(rows, d_model).astype(F32)
    mean = jnp.mean(field * field, axis=-1, keepdims=True)
    normed = (field * lax.rsqrt(mean + EPS) * gain_ref[...]).astype(BF16)
    n_slots = out_refs[0].shape[0]
    for piece, out_ref in enumerate(out_refs):
        slot = iota((n_slots, rows), 0) + piece * n_slots
        picked = slot == slots[0]
        for one in slots[1:]:
            picked = picked | (slot == one)
        picked = picked.astype(F32).astype(BF16)
        out_ref[...] = jnp.dot(picked, normed, preferred_element_type=F32).astype(BF16)


def dispatch(core, ep, tokens, gain, routes, weight, n_z, n_ep, n_local, per):
    local_rows, d_model = tokens.shape
    block = local_rows // (n_z * CORES)
    n_slots = per * n_z * CAP
    n_out = n_ep * (n_local // per)
    whole = lambda a: pl.BlockSpec(a.shape, lambda i, c, e: (0,) * a.ndim)
    outs = pl.pallas_call(
        lambda *refs: dispatch_kernel(n_ep, n_local, per, *refs),
        grid_spec=pltpu.PrefetchScalarGridSpec(
            num_scalar_prefetch=2,
            grid=(1,),
            in_specs=[
                pl.BlockSpec((n_z, 1, block, d_model), lambda i, c, e: (0, c[0], 0, 0)),
                whole(gain),
                whole(routes),
                whole(weight),
            ],
            out_specs=[IN_VMEM] * (n_out + 1),
        ),
        out_shape=[jax.ShapeDtypeStruct((n_slots, d_model), BF16)] * n_out
        + [jax.ShapeDtypeStruct((n_z * block, 8), F32)],
        compiler_params=pltpu.CompilerParams(vmem_limit_bytes=16 * MIB),
        name="dispatch",
    )(core, ep, *in_hbm([tokens.reshape(n_z, CORES, block, d_model), gain, routes, weight]))
    return outs[:n_out], outs[n_out]


def expert_kernel(n_in, group, first, n_next, *refs):
    ins, (gate_ref, up_ref, down_ref) = refs[:n_in], refs[n_in : n_in + 3]
    sources, outs = refs[n_in + 3 : n_in + 3 + n_next], refs[n_in + 3 + n_next : 2 * n_in + 3 + n_next]
    per, rows, _ = outs[0].shape
    copies = []
    if n_next:
        copies = weight_copies(sources, refs[2 * n_in + 3 + n_next : -1], first + per, refs[-1], 0)
    for copy in copies:
        copy.start()
    for expert in range(per):
        for start in range(0, len(ins), group):
            field = [ref[expert] for ref in ins[start : start + group]]
            field = jnp.concatenate(field, axis=0)
            gate = jnp.dot(field, gate_ref[expert], preferred_element_type=F32)
            up = jnp.dot(field, up_ref[expert], preferred_element_type=F32)
            hidden = (gate / (1.0 + jnp.exp(-gate)) * up).astype(BF16)
            result = jnp.dot(hidden, down_ref[expert], preferred_element_type=F32)
            for n, ref in enumerate(outs[start : start + group]):
                ref[expert] = result[n * rows : (n + 1) * rows].astype(BF16)
    for copy in copies:
        copy.wait()


def experts(own, other, weights, first, all_weights):
    pieces = [*own, *other]
    _, rows, d_model = pieces[0].shape
    per = weights[0].shape[0]
    more = in_hbm(all_weights) if first + per < all_weights[0].shape[0] else []
    group = min(len(pieces), max(1, 256 // rows))
    outs = pl.pallas_call(
        lambda *refs: expert_kernel(len(pieces), group, first, len(more), *refs),
        in_specs=[IN_VMEM] * (len(pieces) + 3) + [pl.BlockSpec(memory_space=pl.ANY)] * len(more),
        out_specs=[IN_VMEM] * (len(pieces) + len(more)),
        out_shape=[jax.ShapeDtypeStruct((per, rows, d_model), BF16)] * len(pieces)
        + [jax.ShapeDtypeStruct((per, *w.shape[1:]), BF16) for w in more],
        scratch_shapes=[pltpu.SemaphoreType.DMA((3 * per * SPLIT,))] if more else [],
        compiler_params=pltpu.CompilerParams(vmem_limit_bytes=16 * MIB),
        name="experts",
    )(*pieces, *weights, *more)
    return outs[: len(own)], outs[len(own) : len(pieces)], outs[len(pieces) :]


def combine_kernel(n_back, z_ref, cols_ref, *rest):
    back_refs, out_refs, total_ref = rest[:n_back], rest[n_back:-1], rest[-1]
    rows = cols_ref.shape[0]
    back = jnp.concatenate([ref[...] for ref in back_refs], axis=0)
    slot = lax.broadcasted_iota(jnp.int32, (rows, back.shape[0]), 1)
    matrix = jnp.zeros(slot.shape, F32)
    for k in range(TOPK):
        own = (cols_ref[:, k : k + 1] + 0.5).astype(jnp.int32)
        share = cols_ref[:, TOPK + k : TOPK + k + 1]
        matrix = matrix + jnp.where(slot == own, share, 0.0)
    high = matrix.astype(BF16)
    low = (matrix - high.astype(F32)).astype(BF16)
    both = jnp.dot(jnp.concatenate([high, low], axis=0), back, preferred_element_type=F32)
    total_ref[...] = (both[:rows] + both[rows:]).reshape(total_ref.shape)
    n_z = len(out_refs)
    for n, out_ref in enumerate(out_refs):
        out_ref[...] = total_ref[peer(z_ref[0], n, n_z)].astype(BF16)


def combine(z_index, cols, backs, n_z):
    rows, d_model = cols.shape[0], backs[0].shape[-1]
    return pl.pallas_call(
        lambda *refs: combine_kernel(len(backs), *refs),
        in_specs=[IN_SMEM] + [IN_VMEM] * (1 + len(backs)),
        out_specs=[IN_VMEM] * n_z,
        out_shape=[jax.ShapeDtypeStruct((rows // n_z, d_model), BF16)] * n_z,
        scratch_shapes=[pltpu.VMEM((n_z, rows // n_z, d_model), F32)],
        compiler_params=pltpu.CompilerParams(vmem_limit_bytes=24 * MIB),
        name="combine",
    )(z_index, cols, *backs)


def peer(own, step, n):
    return own ^ step if n & (n - 1) == 0 else lax.rem(own + step, n)


def shift(a, axis, step, back=False):
    n = lax.axis_size(axis)
    if n & (n - 1) == 0:
        pairs = [(i, i ^ step) for i in range(n)]
    else:
        pairs = [(i, (i - step if back else i + step) % n) for i in range(n)]
    return lax.ppermute(a, axis, pairs)


def swap_cores(a):
    return lax.ppermute(a, "core", [(i, CORES - 1 - i) for i in range(CORES)])


def on_device(
    queries,
    keys,
    values,
    query_gain,
    key_gain,
    out_weight,
    tokens_b,
    norm_gain,
    routes,
    route_weight,
    gate_weight,
    up_weight,
    down_weight,
):
    n_ep, n_z = lax.axis_size("ep"), lax.axis_size("z")
    core, z_index = lax.axis_index("core"), lax.axis_index("z")
    core_arg = core.reshape(1).astype(jnp.int32)
    z_arg = z_index.reshape(1).astype(jnp.int32)
    n_rows, width = queries.shape
    d_model = tokens_b.shape[-1]
    heads = width // HD
    n_heads = heads * n_z * CORES

    part = n_rows // (n_z * CORES)
    offsets = (
        jnp.arange(n_z, dtype=jnp.int32)[:, None] * (CORES * part)
        + core * part
        + jnp.arange(part, dtype=jnp.int32)[None, :]
    ).reshape(-1)
    cosine, sine = rope_tables(lax.axis_index("ep") * n_rows + offsets)
    kv_head = ((z_index * CORES + core) * heads // (n_heads // KVH)).reshape(1).astype(jnp.int32)
    own_kv, q_send, q_own = prepare(
        core_arg, kv_head, keys, values, queries, key_gain[None], cosine, sine, n_z
    )
    pieces = [own_kv]
    for step in range(1, n_ep):
        pieces.append(shift(own_kv, "ep", step))
    pieces = pieces + [swap_cores(p) for p in pieces]

    q_other = swap_cores(q_send)
    w_other = swap_cores(out_weight)

    n_local = gate_weight.shape[0]
    chunks = 2 if n_local % 2 == 0 else 1
    per = n_local // chunks
    ep_arg = lax.axis_index("ep").reshape(1).astype(jnp.int32)
    outgoing, cols = dispatch(
        core_arg, ep_arg, tokens_b, norm_gain[None], routes.T, route_weight.T, n_z, n_ep, n_local,
        per,
    )
    arrived = []
    for chunk in range(chunks):
        here = []
        for step in range(n_ep):
            piece = outgoing[chunk * n_ep + step].reshape(per, n_z * CAP, d_model)
            here.append(shift(piece, "ep", step) if step else piece)
        arrived.append((here, [swap_cores(p) for p in here]))

    all_weights = [gate_weight, up_weight, down_weight]
    mixed, weights = mix(
        z_arg, q_own, q_other, query_gain[None], cosine, sine, out_weight, w_other,
        all_weights, per, pieces,
    )
    gathered = [mixed[0]]
    for step in range(1, n_z):
        gathered.append(shift(mixed[step], "z", step))
    mixed_out = add(*gathered)

    backs = []
    for chunk in range(chunks):
        keep, send, weights = experts(*arrived[chunk], weights, chunk * per, all_weights)
        for step in range(n_ep):
            result = add(keep[step], swap_cores(send[step]))
            result = shift(result, "ep", step, back=True) if step else result
            backs.append(result.reshape(-1, d_model))
    rows = combine(z_arg, cols, backs, n_z)
    gathered = [rows[0]]
    for step in range(1, n_z):
        gathered.append(shift(rows[step], "z", step))
    expert_out = add(*gathered)
    return (mixed_out, expert_out)


def solution(mesh):
    n_ep, n_tp = mesh.shape["ep"], mesh.shape["tp"]
    fine = Mesh(mesh.devices.reshape(n_ep, n_tp // CORES, CORES), ("ep", "z", "core"))
    tp = ("z", "core")
    placed = (
        P("ep", tp),
        P("ep", None),
        P("ep", None),
        P(),
        P(),
        P(tp, None),
        P("ep", None),
        P(),
        P("ep", None),
        P("ep", None),
        P("ep", None, tp),
        P("ep", None, tp),
        P("ep", tp, None),
    )

    return jax.shard_map(
        on_device,
        mesh=fine,
        in_specs=placed,
        out_specs=(P(("ep", "z", "core"), None), P(("ep", "z", "core"), None)),
        check_vma=False,
    )
```

```python
import jax
import jax.numpy as jnp
from jax import lax
from jax.experimental import pallas as pl
from jax.experimental.pallas import tpu as pltpu
from jax.sharding import Mesh, PartitionSpec as P


HD = 128
KVH = 4
EXPERTS = 16
TOPK = 2
GRID_W = 64
CAP = 8
EPS = 1e-06
THETA = 10000.0
CORES = 2
IN_VMEM = pl.BlockSpec(memory_space=pltpu.VMEM)
IN_SMEM = pl.BlockSpec(memory_space=pltpu.SMEM)
SPLIT = 2
KEY_CHUNK = 1024
MIB = 1024 * 1024

F32 = jnp.float32
BF16 = jnp.bfloat16


def in_hbm(arrays):
    return [pltpu.with_memory_space_constraint(a, pltpu.HBM) for a in arrays]


def rope_tables(positions):
    n_freq = HD // 4
    row_pos = (positions // GRID_W).astype(F32)[:, None]
    col_pos = (positions % GRID_W).astype(F32)[:, None]
    lane = jnp.arange(HD, dtype=jnp.int32)
    inverse = THETA ** (-(lane % n_freq).astype(F32) / n_freq)
    angle = jnp.where(lane < HD // 2, row_pos, col_pos) * inverse
    sign = jnp.where((lane // n_freq) % 2 == 0, -1.0, 1.0).astype(F32)
    return jnp.cos(angle), jnp.sin(angle) * sign


def norm_turn(field, gain, cosine, sine):
    quarter = HD // 4
    mean = jnp.mean(field * field, axis=-1, keepdims=True)
    field = field * lax.rsqrt(mean + EPS) * gain
    lane = lax.broadcasted_iota(jnp.int32, field.shape, 1)
    partner = jnp.where(
        (lane // quarter) % 2 == 0,
        pltpu.roll(field, HD - quarter, 1),
        pltpu.roll(field, quarter, 1),
    )
    return field * cosine + partner * sine


def prepare_kernel(
    core_ref, head_ref, keys_ref, values_ref, q_ref, own_ref, gain_ref, cos_ref, sin_ref,
    kv_ref, send_ref, keep_ref,
):
    rows = cos_ref.shape[0]
    field = keys_ref[...].reshape(rows, HD).astype(F32)
    kv_ref[0] = norm_turn(field, gain_ref[...], cos_ref[...], sin_ref[...]).astype(BF16)
    kv_ref[1] = values_ref[...].reshape(rows, HD)
    send_ref[...] = q_ref[...].reshape(send_ref.shape)
    keep_ref[...] = own_ref[...].reshape(keep_ref.shape)


def prepare(core, head, keys, values, queries, gain, cosine, sine, n_z):
    rows, width = cosine.shape[0], queries.shape[-1]
    part = rows // n_z
    view = lambda a: a.reshape(n_z, CORES, part, a.shape[-1])
    picked = pl.BlockSpec((n_z, 1, part, HD), lambda i, c, h: (0, c[0], 0, h[0]))
    whole = lambda shape: pl.BlockSpec(shape, lambda i, c, h: (0,) * len(shape))
    return pl.pallas_call(
        prepare_kernel,
        grid_spec=pltpu.PrefetchScalarGridSpec(
            num_scalar_prefetch=2,
            grid=(1,),
            in_specs=[
                picked,
                picked,
                pl.BlockSpec((n_z, 1, part, width), lambda i, c, h: (0, 1 - c[0], 0, 0)),
                pl.BlockSpec((n_z, 1, part, width), lambda i, c, h: (0, c[0], 0, 0)),
                whole((1, HD)),
                whole((rows, HD)),
                whole((rows, HD)),
            ],
            out_specs=[IN_VMEM] * 3,
        ),
        out_shape=[
            jax.ShapeDtypeStruct((2, rows, HD), BF16),
            jax.ShapeDtypeStruct((n_z, part, width), BF16),
            jax.ShapeDtypeStruct((n_z, part, width), BF16),
        ],
        compiler_params=pltpu.CompilerParams(vmem_limit_bytes=8 * MIB),
        name="prepare",
    )(
        core, head, *in_hbm([view(keys), view(values), view(queries), view(queries), gain]),
        cosine, sine,
    )


def add_kernel(*refs):
    total = refs[0][...].astype(F32)
    for ref in refs[1:-1]:
        total = total + ref[...].astype(F32)
    refs[-1][...] = total.astype(BF16)


def add(*arrays):
    return pl.pallas_call(
        add_kernel,
        in_specs=[IN_VMEM] * len(arrays),
        out_specs=IN_VMEM,
        out_shape=jax.ShapeDtypeStruct(arrays[0].shape, BF16),
        compiler_params=pltpu.CompilerParams(vmem_limit_bytes=8 * MIB),
        name="add",
    )(*arrays)


def weight_copies(sources, targets, first, sems, sem):
    copies = []
    for source, target in zip(sources, targets):
        per, rows, _ = target.shape
        cut = rows // SPLIT
        for expert in range(per):
            for n in range(SPLIT):
                part = pl.ds(n * cut, cut)
                copies.append(
                    pltpu.make_async_copy(
                        source.at[first + expert, part], target.at[expert, part], sems.at[sem]
                    )
                )
                sem += 1
    return copies


def load_kernel(first, after_ref, *refs):
    sources, targets, sems = refs[:3], refs[3:6], refs[6]
    copies = weight_copies(sources, targets, first, sems, 0)
    for copy in copies:
        copy.start()
    for copy in copies:
        copy.wait()


def load(weights, first, per, after):
    any_space = pl.BlockSpec(memory_space=pl.ANY)
    return pl.pallas_call(
        lambda *refs: load_kernel(first, *refs),
        in_specs=[any_space] * 4,
        out_specs=[IN_VMEM] * 3,
        out_shape=[jax.ShapeDtypeStruct((per, *w.shape[1:]), BF16) for w in weights],
        scratch_shapes=[pltpu.SemaphoreType.DMA((3 * per * SPLIT,))],
        compiler_params=pltpu.CompilerParams(vmem_limit_bytes=2 * MIB),
        name="load",
    )(after, *in_hbm(weights))


def mix_kernel(n_pieces, n_z, z_ref, q_own, q_other, gain_hbm, cos_ref, sin_ref, w_other, *rest):
    pieces = rest[4 : 4 + n_pieces]
    outs = rest[4 + n_pieces : 4 + n_pieces + n_z]
    loaded = rest[4 + n_pieces + n_z : 7 + n_pieces + n_z]
    keys_ref, vals_ref, mixed_ref, w_own, gain_ref, sems = rest[7 + n_pieces + n_z :]
    copies = [
        pltpu.make_async_copy(gain_hbm, gain_ref, sems.at[0]),
        pltpu.make_async_copy(rest[0], w_own, sems.at[1]),
        *weight_copies(rest[1:4], loaded, 0, sems, 2),
    ]
    for copy in copies:
        copy.start()
    row = 0
    for piece in pieces:
        rows = piece.shape[1]
        keys_ref[row : row + rows] = piece[0]
        vals_ref[row : row + rows, :HD] = piece[1]
        row += rows
    vals_ref[:, HD:] = jnp.ones((row, HD), BF16)
    factor = HD ** (-0.5) * 1.4426950408889634
    part = q_own.shape[1]
    heads = q_own.shape[-1] // HD
    n_chunks = max(1, row // KEY_CHUNK)
    cut = row // n_chunks
    tile = CORES * heads * part // 2

    copies[0].wait()
    copies[1].wait()

    def one(n, carry):
        block = peer(z_ref[0], n, n_z)
        at = pl.multiple_of(block * part, 16)
        cosine, sine = cos_ref[pl.ds(at, part)], sin_ref[pl.ds(at, part)]
        queries = []
        for field in (q_own[block], q_other[block]):
            for head in range(heads):
                vec = field[:, head * HD : (head + 1) * HD].astype(F32)
                queries.append(norm_turn(vec, gain_ref[...], cosine, sine).astype(BF16))
        query = jnp.concatenate(queries, axis=0)
        tiles = [query[:tile], query[tile:]]
        score = lambda side, c: lax.dot_general(
            tiles[side], keys_ref[c * cut : (c + 1) * cut],
            (((1,), (1,)), ((), ())), preferred_element_type=F32,
        )
        work = [(c, side) for c in range(n_chunks) for side in range(2)]
        top, total = [None] * 2, [None] * 2
        scores = score(0, 0)
        for step, (c, side) in enumerate(work):
            after = score(work[step + 1][1], work[step + 1][0]) if step + 1 < len(work) else None
            here = jnp.max(scores, axis=1, keepdims=True)
            if c:
                here = jnp.maximum(top[side], here)
                shrink = jnp.exp2((top[side] - here) * factor)
            weights = jnp.exp2((scores - here) * factor).astype(BF16)
            part_sum = jnp.dot(
                weights, vals_ref[c * cut : (c + 1) * cut], preferred_element_type=F32
            )
            total[side] = total[side] * shrink + part_sum if c else part_sum
            top[side] = here
            scores = after
        mixed = None
        for side, weight in enumerate((w_own, w_other)):
            merged = (total[side][:, :HD] / total[side][:, HD:]).astype(BF16)
            merged = jnp.concatenate(
                [merged[h * part : (h + 1) * part] for h in range(heads)], axis=1
            )
            out = jnp.dot(merged, weight[...], preferred_element_type=F32)
            mixed = out if mixed is None else mixed + out
        mixed_ref[n] = mixed.astype(BF16)
        return carry

    lax.fori_loop(0, n_z, one, 0)
    for n, out_ref in enumerate(outs):
        out_ref[...] = mixed_ref[n]
    for copy in copies[2:]:
        copy.wait()


def mix(z_index, q_own, q_other, gain, cosine, sine, w_own, w_other, weights, per, pieces):
    n_z, part, _ = q_own.shape
    d_model = w_own.shape[-1]
    length = sum(p.shape[1] for p in pieces)
    any_space = pl.BlockSpec(memory_space=pl.ANY)
    outs = pl.pallas_call(
        lambda *refs: mix_kernel(len(pieces), n_z, *refs),
        in_specs=[IN_SMEM, IN_VMEM, IN_VMEM, any_space, IN_VMEM, IN_VMEM, IN_VMEM]
        + [any_space] * 4
        + [IN_VMEM] * len(pieces),
        out_specs=[IN_VMEM] * (n_z + 3),
        out_shape=[jax.ShapeDtypeStruct((part, d_model), BF16)] * n_z
        + [jax.ShapeDtypeStruct((per, *w.shape[1:]), BF16) for w in weights],
        scratch_shapes=[
            pltpu.VMEM((length, HD), BF16),
            pltpu.VMEM((length, 2 * HD), BF16),
            pltpu.VMEM((n_z, part, d_model), BF16),
            pltpu.VMEM(w_own.shape, BF16),
            pltpu.VMEM(gain.shape, F32),
            pltpu.SemaphoreType.DMA((2 + 3 * per * SPLIT,)),
        ],
        compiler_params=pltpu.CompilerParams(vmem_limit_bytes=8 * MIB + length * HD * 6),
        name="mix",
    )(
        z_index, q_own, q_other, *in_hbm([gain]), cosine, sine, w_other,
        *in_hbm([w_own, *weights]), *pieces,
    )
    return outs[:n_z], outs[n_z:]


def block_of(index, block, count):
    found = jnp.zeros_like(index)
    for n in range(1, count):
        found = found + (index >= n * block).astype(jnp.int32)
    return found


def dispatch_kernel(
    n_ep, n_local, per, core_ref, ep_ref, tokens_ref, gain_ref, routes_ref, weight_ref, *rest
):
    out_refs, cols_ref = rest[:-1], rest[-1]
    n_z, _, block, d_model = tokens_ref.shape
    rows, local_rows = n_z * block, routes_ref.shape[1]
    iota = lambda shape, dim: lax.broadcasted_iota(jnp.int32, shape, dim)
    exact = dict(preferred_element_type=F32, precision=lax.Precision.HIGHEST)

    lane = iota((local_rows, rows), 1)
    lane_block = block_of(lane, block, n_z)
    source = lane + (lane_block * (CORES - 1) + core_ref[0]) * block
    select = (iota((local_rows, rows), 0) == source).astype(F32)
    chosen = jnp.dot(routes_ref[...].astype(F32), select, **exact)
    chosen = (chosen + 0.5).astype(jnp.int32)
    weight = jnp.dot(weight_ref[...], select, **exact)

    shape = (EXPERTS, rows)
    expert = iota(shape, 0)
    hot = [expert == chosen[k : k + 1] for k in range(TOPK)]
    either = hot[0]
    for one in hot[1:]:
        either = either | one
    square = (rows, rows)
    above, across = iota(square, 0), iota(square, 1)
    first = block_of(across, block, n_z) * block
    earlier = ((above < across) & (above >= first)).astype(F32).astype(BF16)
    count = jnp.dot(either.astype(F32).astype(BF16), earlier, preferred_element_type=F32)
    owner = block_of(expert, n_local, n_ep)
    if n_ep & (n_ep - 1) == 0:
        ahead = owner ^ ep_ref[0]
    else:
        ahead = owner - ep_ref[0]
        ahead = jnp.where(ahead < 0, ahead + n_ep, ahead)
    local = expert - owner * n_local
    turn = block_of(local, per, n_local // per)
    place = ((turn * n_ep + ahead) * per + local - turn * per) * (n_z * CAP)
    place = place + block_of(iota(shape, 1), block, n_z) * CAP + (count + 0.5).astype(jnp.int32)
    slots = [jnp.sum(jnp.where(h, place, 0), axis=0, keepdims=True) for h in hot]

    total = jnp.sum(weight, axis=0, keepdims=True)
    table = [s.astype(F32) for s in slots] + [weight[k : k + 1] / total for k in range(TOPK)]
    lines = iota((8, rows), 0)
    stacked = jnp.zeros((8, rows), F32)
    for n, line in enumerate(table):
        stacked = jnp.where(lines == n, line, stacked)
    same = (above == across).astype(F32)
    cols_ref[...] = lax.dot_general(same, stacked, (((1,), (1,)), ((), ())), **exact)

    field = tokens_ref[...].reshape(rows, d_model).astype(F32)
    mean = jnp.mean(field * field, axis=-1, keepdims=True)
    normed = (field * lax.rsqrt(mean + EPS) * gain_ref[...]).astype(BF16)
    n_slots = out_refs[0].shape[0]
    for piece, out_ref in enumerate(out_refs):
        slot = iota((n_slots, rows), 0) + piece * n_slots
        picked = slot == slots[0]
        for one in slots[1:]:
            picked = picked | (slot == one)
        picked = picked.astype(F32).astype(BF16)
        out_ref[...] = jnp.dot(picked, normed, preferred_element_type=F32).astype(BF16)


def dispatch(core, ep, tokens, gain, routes, weight, n_z, n_ep, n_local, per):
    local_rows, d_model = tokens.shape
    block = local_rows // (n_z * CORES)
    n_slots = per * n_z * CAP
    n_out = n_ep * (n_local // per)
    whole = lambda a: pl.BlockSpec(a.shape, lambda i, c, e: (0,) * a.ndim)
    outs = pl.pallas_call(
        lambda *refs: dispatch_kernel(n_ep, n_local, per, *refs),
        grid_spec=pltpu.PrefetchScalarGridSpec(
            num_scalar_prefetch=2,
            grid=(1,),
            in_specs=[
                pl.BlockSpec((n_z, 1, block, d_model), lambda i, c, e: (0, c[0], 0, 0)),
                whole(gain),
                whole(routes),
                whole(weight),
            ],
            out_specs=[IN_VMEM] * (n_out + 1),
        ),
        out_shape=[jax.ShapeDtypeStruct((n_slots, d_model), BF16)] * n_out
        + [jax.ShapeDtypeStruct((n_z * block, 8), F32)],
        compiler_params=pltpu.CompilerParams(vmem_limit_bytes=16 * MIB),
        name="dispatch",
    )(core, ep, *in_hbm([tokens.reshape(n_z, CORES, block, d_model), gain, routes, weight]))
    return outs[:n_out], outs[n_out]


def expert_kernel(n_in, group, *refs):
    ins, (gate_ref, up_ref, down_ref) = refs[:n_in], refs[n_in : n_in + 3]
    outs = refs[n_in + 3 :]
    per, rows, _ = outs[0].shape
    for expert in range(per):
        for start in range(0, len(ins), group):
            field = [ref[expert] for ref in ins[start : start + group]]
            field = jnp.concatenate(field, axis=0)
            gate = jnp.dot(field, gate_ref[expert], preferred_element_type=F32)
            up = jnp.dot(field, up_ref[expert], preferred_element_type=F32)
            hidden = (gate / (1.0 + jnp.exp(-gate)) * up).astype(BF16)
            result = jnp.dot(hidden, down_ref[expert], preferred_element_type=F32)
            for n, ref in enumerate(outs[start : start + group]):
                ref[expert] = result[n * rows : (n + 1) * rows].astype(BF16)


def experts(own, other, weights):
    pieces = [*own, *other]
    _, rows, d_model = pieces[0].shape
    per = weights[0].shape[0]
    group = min(len(pieces), max(1, 256 // rows))
    outs = pl.pallas_call(
        lambda *refs: expert_kernel(len(pieces), group, *refs),
        in_specs=[IN_VMEM] * (len(pieces) + 3),
        out_specs=[IN_VMEM] * len(pieces),
        out_shape=[jax.ShapeDtypeStruct((per, rows, d_model), BF16)] * len(pieces),
        compiler_params=pltpu.CompilerParams(vmem_limit_bytes=10 * MIB),
        name="experts",
    )(*pieces, *weights)
    return outs[: len(own)], outs[len(own) :]


def combine_kernel(n_back, z_ref, cols_ref, *rest):
    back_refs, out_refs, total_ref = rest[:n_back], rest[n_back:-1], rest[-1]
    rows = cols_ref.shape[0]
    back = jnp.concatenate([ref[...] for ref in back_refs], axis=0)
    slot = lax.broadcasted_iota(jnp.int32, (rows, back.shape[0]), 1)
    matrix = jnp.zeros(slot.shape, F32)
    for k in range(TOPK):
        own = (cols_ref[:, k : k + 1] + 0.5).astype(jnp.int32)
        share = cols_ref[:, TOPK + k : TOPK + k + 1]
        matrix = matrix + jnp.where(slot == own, share, 0.0)
    high = matrix.astype(BF16)
    low = (matrix - high.astype(F32)).astype(BF16)
    both = jnp.dot(jnp.concatenate([high, low], axis=0), back, preferred_element_type=F32)
    total_ref[...] = (both[:rows] + both[rows:]).reshape(total_ref.shape)
    n_z = len(out_refs)
    for n, out_ref in enumerate(out_refs):
        out_ref[...] = total_ref[peer(z_ref[0], n, n_z)].astype(BF16)


def combine(z_index, cols, backs, n_z):
    rows, d_model = cols.shape[0], backs[0].shape[-1]
    return pl.pallas_call(
        lambda *refs: combine_kernel(len(backs), *refs),
        in_specs=[IN_SMEM] + [IN_VMEM] * (1 + len(backs)),
        out_specs=[IN_VMEM] * n_z,
        out_shape=[jax.ShapeDtypeStruct((rows // n_z, d_model), BF16)] * n_z,
        scratch_shapes=[pltpu.VMEM((n_z, rows // n_z, d_model), F32)],
        compiler_params=pltpu.CompilerParams(vmem_limit_bytes=24 * MIB),
        name="combine",
    )(z_index, cols, *backs)


def peer(own, step, n):
    return own ^ step if n & (n - 1) == 0 else lax.rem(own + step, n)


def shift(a, axis, step, back=False):
    n = lax.axis_size(axis)
    if n & (n - 1) == 0:
        pairs = [(i, i ^ step) for i in range(n)]
    else:
        pairs = [(i, (i - step if back else i + step) % n) for i in range(n)]
    return lax.ppermute(a, axis, pairs)


def swap_cores(a):
    return lax.ppermute(a, "core", [(i, CORES - 1 - i) for i in range(CORES)])


def on_device(
    queries,
    keys,
    values,
    query_gain,
    key_gain,
    out_weight,
    tokens_b,
    norm_gain,
    routes,
    route_weight,
    gate_weight,
    up_weight,
    down_weight,
):
    n_ep, n_z = lax.axis_size("ep"), lax.axis_size("z")
    core, z_index = lax.axis_index("core"), lax.axis_index("z")
    core_arg = core.reshape(1).astype(jnp.int32)
    z_arg = z_index.reshape(1).astype(jnp.int32)
    n_rows, width = queries.shape
    d_model = tokens_b.shape[-1]
    heads = width // HD
    n_heads = heads * n_z * CORES

    part = n_rows // (n_z * CORES)
    offsets = (
        jnp.arange(n_z, dtype=jnp.int32)[:, None] * (CORES * part)
        + core * part
        + jnp.arange(part, dtype=jnp.int32)[None, :]
    ).reshape(-1)
    cosine, sine = rope_tables(lax.axis_index("ep") * n_rows + offsets)
    kv_head = ((z_index * CORES + core) * heads // (n_heads // KVH)).reshape(1).astype(jnp.int32)
    own_kv, q_send, q_own = prepare(
        core_arg, kv_head, keys, values, queries, key_gain[None], cosine, sine, n_z
    )
    pieces = [own_kv]
    for step in range(1, n_ep):
        pieces.append(shift(own_kv, "ep", step))
    pieces = pieces + [swap_cores(p) for p in pieces]

    q_other = swap_cores(q_send)
    w_other = swap_cores(out_weight)

    n_local = gate_weight.shape[0]
    chunks = 2 if n_local % 2 == 0 else 1
    per = n_local // chunks
    ep_arg = lax.axis_index("ep").reshape(1).astype(jnp.int32)
    outgoing, cols = dispatch(
        core_arg, ep_arg, tokens_b, norm_gain[None], routes.T, route_weight.T, n_z, n_ep, n_local,
        per,
    )
    arrived = []
    for chunk in range(chunks):
        here = []
        for step in range(n_ep):
            piece = outgoing[chunk * n_ep + step].reshape(per, n_z * CAP, d_model)
            here.append(shift(piece, "ep", step) if step else piece)
        arrived.append((here, [swap_cores(p) for p in here]))

    all_weights = [gate_weight, up_weight, down_weight]
    weights = [load(all_weights, chunk * per, per, cols) for chunk in range(1, chunks)]
    mixed, first_weights = mix(
        z_arg, q_own, q_other, query_gain[None], cosine, sine, out_weight, w_other,
        all_weights, per, pieces,
    )
    weights = [first_weights, *weights]
    gathered = [mixed[0]]
    for step in range(1, n_z):
        gathered.append(shift(mixed[step], "z", step))
    mixed_out = add(*gathered)

    backs = []
    for chunk in range(chunks):
        keep, send = experts(*arrived[chunk], weights[chunk])
        for step in range(n_ep):
            result = add(keep[step], swap_cores(send[step]))
            result = shift(result, "ep", step, back=True) if step else result
            backs.append(result.reshape(-1, d_model))
    rows = combine(z_arg, cols, backs, n_z)
    gathered = [rows[0]]
    for step in range(1, n_z):
        gathered.append(shift(rows[step], "z", step))
    expert_out = add(*gathered)
    return (mixed_out, expert_out)


def solution(mesh):
    n_ep, n_tp = mesh.shape["ep"], mesh.shape["tp"]
    fine = Mesh(mesh.devices.reshape(n_ep, n_tp // CORES, CORES), ("ep", "z", "core"))
    tp = ("z", "core")
    placed = (
        P("ep", tp),
        P("ep", None),
        P("ep", None),
        P(),
        P(),
        P(tp, None),
        P("ep", None),
        P(),
        P("ep", None),
        P("ep", None),
        P("ep", None, tp),
        P("ep", None, tp),
        P("ep", tp, None),
    )

    return jax.shard_map(
        on_device,
        mesh=fine,
        in_specs=placed,
        out_specs=(P(("ep", "z", "core"), None), P(("ep", "z", "core"), None)),
        check_vma=False,
    )
```

```python
import jax
import jax.numpy as jnp
from jax import lax
from jax.experimental import pallas as pl
from jax.experimental.pallas import tpu as pltpu
from jax.sharding import Mesh, PartitionSpec as P


HD = 128
KVH = 4
EXPERTS = 16
TOPK = 2
GRID_W = 64
CAP = 8
EPS = 1e-06
THETA = 10000.0
CORES = 2
IN_VMEM = pl.BlockSpec(memory_space=pltpu.VMEM)
IN_SMEM = pl.BlockSpec(memory_space=pltpu.SMEM)
SPLIT = 2
KEY_CHUNK = 1024
MIB = 1024 * 1024

F32 = jnp.float32
BF16 = jnp.bfloat16


def in_hbm(arrays):
    return [pltpu.with_memory_space_constraint(a, pltpu.HBM) for a in arrays]


def rope_tables(positions):
    n_freq = HD // 4
    row_pos = (positions // GRID_W).astype(F32)[:, None]
    col_pos = (positions % GRID_W).astype(F32)[:, None]
    lane = jnp.arange(HD, dtype=jnp.int32)
    inverse = THETA ** (-(lane % n_freq).astype(F32) / n_freq)
    angle = jnp.where(lane < HD // 2, row_pos, col_pos) * inverse
    sign = jnp.where((lane // n_freq) % 2 == 0, -1.0, 1.0).astype(F32)
    return jnp.cos(angle), jnp.sin(angle) * sign


def norm_turn(field, gain, cosine, sine):
    quarter = HD // 4
    mean = jnp.mean(field * field, axis=-1, keepdims=True)
    field = field * lax.rsqrt(mean + EPS) * gain
    lane = lax.broadcasted_iota(jnp.int32, field.shape, 1)
    partner = jnp.where(
        (lane // quarter) % 2 == 0,
        pltpu.roll(field, HD - quarter, 1),
        pltpu.roll(field, quarter, 1),
    )
    return field * cosine + partner * sine


def prepare_kernel(
    core_ref, head_ref, keys_ref, values_ref, q_ref, own_ref, gain_ref, cos_ref, sin_ref,
    kv_ref, send_ref, keep_ref,
):
    rows = cos_ref.shape[0]
    field = keys_ref[...].reshape(rows, HD).astype(F32)
    kv_ref[0] = norm_turn(field, gain_ref[...], cos_ref[...], sin_ref[...]).astype(BF16)
    kv_ref[1] = values_ref[...].reshape(rows, HD)
    send_ref[...] = q_ref[...].reshape(send_ref.shape)
    keep_ref[...] = own_ref[...].reshape(keep_ref.shape)


def prepare(core, head, keys, values, queries, gain, cosine, sine, n_z):
    rows, width = cosine.shape[0], queries.shape[-1]
    part = rows // n_z
    view = lambda a: a.reshape(n_z, CORES, part, a.shape[-1])
    picked = pl.BlockSpec((n_z, 1, part, HD), lambda i, c, h: (0, c[0], 0, h[0]))
    whole = lambda shape: pl.BlockSpec(shape, lambda i, c, h: (0,) * len(shape))
    return pl.pallas_call(
        prepare_kernel,
        grid_spec=pltpu.PrefetchScalarGridSpec(
            num_scalar_prefetch=2,
            grid=(1,),
            in_specs=[
                picked,
                picked,
                pl.BlockSpec((n_z, 1, part, width), lambda i, c, h: (0, 1 - c[0], 0, 0)),
                pl.BlockSpec((n_z, 1, part, width), lambda i, c, h: (0, c[0], 0, 0)),
                whole((1, HD)),
                whole((rows, HD)),
                whole((rows, HD)),
            ],
            out_specs=[IN_VMEM] * 3,
        ),
        out_shape=[
            jax.ShapeDtypeStruct((2, rows, HD), BF16),
            jax.ShapeDtypeStruct((n_z, part, width), BF16),
            jax.ShapeDtypeStruct((n_z, part, width), BF16),
        ],
        compiler_params=pltpu.CompilerParams(vmem_limit_bytes=8 * MIB),
        name="prepare",
    )(
        core, head, *in_hbm([view(keys), view(values), view(queries), view(queries), gain]),
        cosine, sine,
    )


def add_kernel(n_out, *refs):
    ins, outs = refs[:-n_out], refs[-n_out:]
    total = ins[0][...].astype(F32)
    for ref in ins[1:]:
        total = total + ref[...].astype(F32)
    width = outs[0].shape[-1]
    for n, ref in enumerate(outs):
        ref[...] = total[..., n * width : (n + 1) * width].astype(BF16)


def add(*arrays, halves=1):
    *lead, width = arrays[0].shape
    out = jax.ShapeDtypeStruct((*lead, width // halves), BF16)
    return pl.pallas_call(
        lambda *refs: add_kernel(halves, *refs),
        in_specs=[IN_VMEM] * len(arrays),
        out_specs=[IN_VMEM] * halves,
        out_shape=[out] * halves,
        compiler_params=pltpu.CompilerParams(vmem_limit_bytes=8 * MIB),
        name="add",
    )(*arrays)


def join_kernel(*refs):
    ins, out_ref = refs[:-1], refs[-1]
    width = ins[0].shape[-1]
    count = out_ref.shape[-1] // width
    for n in range(count):
        total = ins[n][...].astype(F32)
        for ref in ins[n + count :: count]:
            total = total + ref[...].astype(F32)
        out_ref[:, n * width : (n + 1) * width] = total.astype(BF16)


def join(parts):
    flat = [h for part in parts for h in part]
    rows, width = flat[0].shape
    return pl.pallas_call(
        join_kernel,
        in_specs=[IN_VMEM] * len(flat),
        out_specs=IN_VMEM,
        out_shape=jax.ShapeDtypeStruct((rows, width * len(parts[0])), BF16),
        compiler_params=pltpu.CompilerParams(vmem_limit_bytes=8 * MIB),
        name="join",
    )(*flat)


def weight_copies(sources, targets, first, sems, sem):
    copies = []
    for source, target in zip(sources, targets):
        per, rows, _ = target.shape
        cut = rows // SPLIT
        for expert in range(per):
            for n in range(SPLIT):
                part = pl.ds(n * cut, cut)
                copies.append(
                    pltpu.make_async_copy(
                        source.at[first + expert, part], target.at[expert, part], sems.at[sem]
                    )
                )
                sem += 1
    return copies


def load_kernel(first, after_ref, *refs):
    sources, targets, sems = refs[:3], refs[3:6], refs[6]
    copies = weight_copies(sources, targets, first, sems, 0)
    for copy in copies:
        copy.start()
    for copy in copies:
        copy.wait()


def load(weights, first, per, after):
    any_space = pl.BlockSpec(memory_space=pl.ANY)
    return pl.pallas_call(
        lambda *refs: load_kernel(first, *refs),
        in_specs=[any_space] * 4,
        out_specs=[IN_VMEM] * 3,
        out_shape=[jax.ShapeDtypeStruct((per, *w.shape[1:]), BF16) for w in weights],
        scratch_shapes=[pltpu.SemaphoreType.DMA((3 * per * SPLIT,))],
        compiler_params=pltpu.CompilerParams(vmem_limit_bytes=2 * MIB),
        name="load",
    )(after, *in_hbm(weights))


def mix_kernel(n_pieces, steps, n_loads, z_ref, q_own, q_other, gain_hbm, cos_ref, sin_ref, *rest):
    n_z = q_own.shape[0]
    w_other, w_hbm = rest[:2]
    pieces = rest[2 : 2 + n_pieces]
    sources = rest[2 + n_pieces : 2 + n_pieces + n_loads]
    outs = rest[2 + n_pieces + n_loads : -4]
    mixed_ref, w_own, gain_ref, sems = rest[-4:]
    n_out = len(steps)
    loaded = outs[n_out : n_out + n_loads]
    copies = [
        pltpu.make_async_copy(gain_hbm, gain_ref, sems.at[0]),
        pltpu.make_async_copy(w_hbm, w_own, sems.at[1]),
        *weight_copies(sources, loaded, 0, sems, 2),
    ]
    for copy in copies:
        copy.start()
    if len(outs) > n_out + n_loads:
        keys_ref, vals_ref = outs[n_out + n_loads :]
        row = 0
        for piece in pieces:
            rows = piece.shape[1]
            keys_ref[row : row + rows] = piece[0]
            vals_ref[row : row + rows, :HD] = piece[1]
            row += rows
        vals_ref[:, HD:] = jnp.ones((row, HD), BF16)
    else:
        keys_ref, vals_ref = pieces
        row = keys_ref.shape[0]
    factor = HD ** (-0.5) * 1.4426950408889634
    part = q_own.shape[1]
    heads = q_own.shape[-1] // HD
    n_chunks = max(1, row // KEY_CHUNK)
    cut = row // n_chunks
    tile = CORES * heads * part // 2

    copies[0].wait()
    copies[1].wait()

    def one(n, carry):
        block = peer(z_ref[0], n + steps[0], n_z)
        at = pl.multiple_of(block * part, 16)
        cosine, sine = cos_ref[pl.ds(at, part)], sin_ref[pl.ds(at, part)]
        queries = []
        for field in (q_own[block], q_other[block]):
            for head in range(heads):
                vec = field[:, head * HD : (head + 1) * HD].astype(F32)
                queries.append(norm_turn(vec, gain_ref[...], cosine, sine).astype(BF16))
        query = jnp.concatenate(queries, axis=0)
        tiles = [query[:tile], query[tile:]]
        score = lambda side, c: lax.dot_general(
            tiles[side], keys_ref[c * cut : (c + 1) * cut],
            (((1,), (1,)), ((), ())), preferred_element_type=F32,
        )
        work = [(c, side) for c in range(n_chunks) for side in range(2)]
        top, total = [None] * 2, [None] * 2
        scores = score(0, 0)
        for step, (c, side) in enumerate(work):
            after = score(work[step + 1][1], work[step + 1][0]) if step + 1 < len(work) else None
            here = jnp.max(scores, axis=1, keepdims=True)
            if c:
                here = jnp.maximum(top[side], here)
                shrink = jnp.exp2((top[side] - here) * factor)
            weights = jnp.exp2((scores - here) * factor).astype(BF16)
            part_sum = jnp.dot(
                weights, vals_ref[c * cut : (c + 1) * cut], preferred_element_type=F32
            )
            total[side] = total[side] * shrink + part_sum if c else part_sum
            top[side] = here
            scores = after
        mixed = None
        for side, weight in enumerate((w_own, w_other)):
            merged = (total[side][:, :HD] / total[side][:, HD:]).astype(BF16)
            merged = jnp.concatenate(
                [merged[h * part : (h + 1) * part] for h in range(heads)], axis=1
            )
            out = jnp.dot(merged, weight[...], preferred_element_type=F32)
            mixed = out if mixed is None else mixed + out
        mixed_ref[n] = mixed.astype(BF16)
        return carry

    lax.fori_loop(0, n_out, one, 0)
    for n, out_ref in enumerate(outs[:n_out]):
        out_ref[...] = mixed_ref[n]
    for copy in copies[2:]:
        copy.wait()


def mix(z_index, q_own, q_other, gain, cosine, sine, w_own, w_other, pieces, steps, loads, per):
    _, part, _ = q_own.shape
    d_model = w_own.shape[-1]
    joined = len(pieces) == 2
    length = pieces[0].shape[0] if joined else sum(p.shape[1] for p in pieces)
    whole = [] if joined else [(length, HD), (length, 2 * HD)]
    any_space = pl.BlockSpec(memory_space=pl.ANY)
    shapes = [(part, d_model)] * len(steps) + [(per, *w.shape[1:]) for w in loads] + whole
    outs = pl.pallas_call(
        lambda *refs: mix_kernel(len(pieces), steps, len(loads), *refs),
        in_specs=[IN_SMEM, IN_VMEM, IN_VMEM, any_space, IN_VMEM, IN_VMEM, IN_VMEM, any_space]
        + [IN_VMEM] * len(pieces)
        + [any_space] * len(loads),
        out_specs=[IN_VMEM] * len(shapes),
        out_shape=[jax.ShapeDtypeStruct(shape, BF16) for shape in shapes],
        scratch_shapes=[
            pltpu.VMEM((len(steps), part, d_model), BF16),
            pltpu.VMEM(w_own.shape, BF16),
            pltpu.VMEM(gain.shape, F32),
            pltpu.SemaphoreType.DMA((2 + len(loads) * per * SPLIT,)),
        ],
        compiler_params=pltpu.CompilerParams(vmem_limit_bytes=10 * MIB),
        name="mix",
    )(
        z_index, q_own, q_other, *in_hbm([gain]), cosine, sine, w_other, *in_hbm([w_own]),
        *pieces, *in_hbm(loads),
    )
    at = len(steps)
    return outs[:at], outs[at : at + len(loads)], outs[at + len(loads) :]


def block_of(index, block, count):
    found = jnp.zeros_like(index)
    for n in range(1, count):
        found = found + (index >= n * block).astype(jnp.int32)
    return found


def dispatch_kernel(
    n_ep, n_local, per, core_ref, ep_ref, tokens_ref, gain_ref, routes_ref, weight_ref, *rest
):
    out_refs, cols_ref = rest[:-1], rest[-1]
    n_z, _, block, d_model = tokens_ref.shape
    rows, local_rows = n_z * block, routes_ref.shape[1]
    iota = lambda shape, dim: lax.broadcasted_iota(jnp.int32, shape, dim)
    exact = dict(preferred_element_type=F32, precision=lax.Precision.HIGHEST)

    lane = iota((local_rows, rows), 1)
    lane_block = block_of(lane, block, n_z)
    source = lane + (lane_block * (CORES - 1) + core_ref[0]) * block
    select = (iota((local_rows, rows), 0) == source).astype(F32)
    chosen = jnp.dot(routes_ref[...].astype(F32), select, **exact)
    chosen = (chosen + 0.5).astype(jnp.int32)
    weight = jnp.dot(weight_ref[...], select, **exact)

    shape = (EXPERTS, rows)
    expert = iota(shape, 0)
    hot = [expert == chosen[k : k + 1] for k in range(TOPK)]
    either = hot[0]
    for one in hot[1:]:
        either = either | one
    square = (rows, rows)
    above, across = iota(square, 0), iota(square, 1)
    first = block_of(across, block, n_z) * block
    earlier = ((above < across) & (above >= first)).astype(F32).astype(BF16)
    count = jnp.dot(either.astype(F32).astype(BF16), earlier, preferred_element_type=F32)
    owner = block_of(expert, n_local, n_ep)
    if n_ep & (n_ep - 1) == 0:
        ahead = owner ^ ep_ref[0]
    else:
        ahead = owner - ep_ref[0]
        ahead = jnp.where(ahead < 0, ahead + n_ep, ahead)
    local = expert - owner * n_local
    turn = block_of(local, per, n_local // per)
    place = ((turn * n_ep + ahead) * per + local - turn * per) * (n_z * CAP)
    place = place + block_of(iota(shape, 1), block, n_z) * CAP + (count + 0.5).astype(jnp.int32)
    slots = [jnp.sum(jnp.where(h, place, 0), axis=0, keepdims=True) for h in hot]

    total = jnp.sum(weight, axis=0, keepdims=True)
    table = [s.astype(F32) for s in slots] + [weight[k : k + 1] / total for k in range(TOPK)]
    lines = iota((8, rows), 0)
    stacked = jnp.zeros((8, rows), F32)
    for n, line in enumerate(table):
        stacked = jnp.where(lines == n, line, stacked)
    same = (above == across).astype(F32)
    cols_ref[...] = lax.dot_general(same, stacked, (((1,), (1,)), ((), ())), **exact)

    field = tokens_ref[...].reshape(rows, d_model).astype(F32)
    mean = jnp.mean(field * field, axis=-1, keepdims=True)
    normed = (field * lax.rsqrt(mean + EPS) * gain_ref[...]).astype(BF16)
    n_slots = out_refs[0].shape[0]
    for piece, out_ref in enumerate(out_refs):
        slot = iota((n_slots, rows), 0) + piece * n_slots
        picked = slot == slots[0]
        for one in slots[1:]:
            picked = picked | (slot == one)
        picked = picked.astype(F32).astype(BF16)
        out_ref[...] = jnp.dot(picked, normed, preferred_element_type=F32).astype(BF16)


def dispatch(core, ep, tokens, gain, routes, weight, n_z, n_ep, n_local, per):
    local_rows, d_model = tokens.shape
    block = local_rows // (n_z * CORES)
    n_slots = per * n_z * CAP
    n_out = n_ep * (n_local // per)
    whole = lambda a: pl.BlockSpec(a.shape, lambda i, c, e: (0,) * a.ndim)
    outs = pl.pallas_call(
        lambda *refs: dispatch_kernel(n_ep, n_local, per, *refs),
        grid_spec=pltpu.PrefetchScalarGridSpec(
            num_scalar_prefetch=2,
            grid=(1,),
            in_specs=[
                pl.BlockSpec((n_z, 1, block, d_model), lambda i, c, e: (0, c[0], 0, 0)),
                whole(gain),
                whole(routes),
                whole(weight),
            ],
            out_specs=[IN_VMEM] * (n_out + 1),
        ),
        out_shape=[jax.ShapeDtypeStruct((n_slots, d_model), BF16)] * n_out
        + [jax.ShapeDtypeStruct((n_z * block, 8), F32)],
        compiler_params=pltpu.CompilerParams(vmem_limit_bytes=16 * MIB),
        name="dispatch",
    )(core, ep, *in_hbm([tokens.reshape(n_z, CORES, block, d_model), gain, routes, weight]))
    return outs[:n_out], outs[n_out]


def expert_kernel(n_in, group, *refs):
    ins, (gate_ref, up_ref, down_ref) = refs[:n_in], refs[n_in : n_in + 3]
    outs = refs[n_in + 3 :]
    per, rows, _ = outs[0].shape
    for expert in range(per):
        for start in range(0, len(ins), group):
            field = [ref[expert] for ref in ins[start : start + group]]
            field = jnp.concatenate(field, axis=0)
            gate = jnp.dot(field, gate_ref[expert], preferred_element_type=F32)
            up = jnp.dot(field, up_ref[expert], preferred_element_type=F32)
            hidden = (gate / (1.0 + jnp.exp(-gate)) * up).astype(BF16)
            result = jnp.dot(hidden, down_ref[expert], preferred_element_type=F32)
            for n, ref in enumerate(outs[start : start + group]):
                ref[expert] = result[n * rows : (n + 1) * rows].astype(BF16)


def experts(own, other, weights):
    pieces = [*own, *other]
    _, rows, d_model = pieces[0].shape
    per = weights[0].shape[0]
    group = min(len(pieces), max(1, 256 // rows))
    outs = pl.pallas_call(
        lambda *refs: expert_kernel(len(pieces), group, *refs),
        in_specs=[IN_VMEM] * (len(pieces) + 3),
        out_specs=[IN_VMEM] * len(pieces),
        out_shape=[jax.ShapeDtypeStruct((per, rows, d_model), BF16)] * len(pieces),
        compiler_params=pltpu.CompilerParams(vmem_limit_bytes=10 * MIB),
        name="experts",
    )(*pieces, *weights)
    return outs[: len(own)], outs[len(own) :]


def combine_kernel(n_back, at, z_ref, cols_ref, *rest):
    back_refs, out_refs, total_ref = rest[:n_back], rest[n_back:-1], rest[-1]
    rows = cols_ref.shape[0]
    width = total_ref.shape[-1]
    back = [ref[:, at : at + width] if ref.shape[-1] > width else ref[...] for ref in back_refs]
    back = jnp.concatenate(back, axis=0)
    slot = lax.broadcasted_iota(jnp.int32, (rows, back.shape[0]), 1)
    matrix = jnp.zeros(slot.shape, F32)
    for k in range(TOPK):
        own = (cols_ref[:, k : k + 1] + 0.5).astype(jnp.int32)
        share = cols_ref[:, TOPK + k : TOPK + k + 1]
        matrix = matrix + jnp.where(slot == own, share, 0.0)
    high = matrix.astype(BF16)
    low = (matrix - high.astype(F32)).astype(BF16)
    both = jnp.dot(jnp.concatenate([high, low], axis=0), back, preferred_element_type=F32)
    total_ref[...] = (both[:rows] + both[rows:]).reshape(total_ref.shape)
    n_z = len(out_refs)
    for n, out_ref in enumerate(out_refs):
        out_ref[...] = total_ref[peer(z_ref[0], n, n_z)].astype(BF16)


def combine(z_index, cols, backs, n_z, at, width):
    rows = cols.shape[0]
    return pl.pallas_call(
        lambda *refs: combine_kernel(len(backs), at, *refs),
        in_specs=[IN_SMEM] + [IN_VMEM] * (1 + len(backs)),
        out_specs=[IN_VMEM] * n_z,
        out_shape=[jax.ShapeDtypeStruct((rows // n_z, width), BF16)] * n_z,
        scratch_shapes=[pltpu.VMEM((n_z, rows // n_z, width), F32)],
        compiler_params=pltpu.CompilerParams(vmem_limit_bytes=24 * MIB),
        name="combine",
    )(z_index, cols, *backs)


def chunks_of(n_local):
    return 2 if n_local % 2 == 0 else 1


def peer(own, step, n):
    return own ^ step if n & (n - 1) == 0 else lax.rem(own + step, n)


def shift(a, axis, step, back=False):
    n = lax.axis_size(axis)
    if n & (n - 1) == 0:
        pairs = [(i, i ^ step) for i in range(n)]
    else:
        pairs = [(i, (i - step if back else i + step) % n) for i in range(n)]
    return lax.ppermute(a, axis, pairs)


def swap_cores(a):
    return lax.ppermute(a, "core", [(i, CORES - 1 - i) for i in range(CORES)])


def on_device(
    queries,
    keys,
    values,
    query_gain,
    key_gain,
    out_weight,
    tokens_b,
    norm_gain,
    routes,
    route_weight,
    gate_weight,
    up_weight,
    down_weight,
):
    n_ep, n_z = lax.axis_size("ep"), lax.axis_size("z")
    core, z_index = lax.axis_index("core"), lax.axis_index("z")
    core_arg = core.reshape(1).astype(jnp.int32)
    z_arg = z_index.reshape(1).astype(jnp.int32)
    n_rows, width = queries.shape
    d_model = tokens_b.shape[-1]
    heads = width // HD
    n_heads = heads * n_z * CORES

    part = n_rows // (n_z * CORES)
    offsets = (
        jnp.arange(n_z, dtype=jnp.int32)[:, None] * (CORES * part)
        + core * part
        + jnp.arange(part, dtype=jnp.int32)[None, :]
    ).reshape(-1)
    cosine, sine = rope_tables(lax.axis_index("ep") * n_rows + offsets)
    kv_head = ((z_index * CORES + core) * heads // (n_heads // KVH)).reshape(1).astype(jnp.int32)
    own_kv, q_send, q_own = prepare(
        core_arg, kv_head, keys, values, queries, key_gain[None], cosine, sine, n_z
    )
    pieces = [own_kv]
    for step in range(1, n_ep):
        pieces.append(shift(own_kv, "ep", step))
    pieces = pieces + [swap_cores(p) for p in pieces]

    q_other = swap_cores(q_send)
    w_other = swap_cores(out_weight)

    n_local = gate_weight.shape[0]
    chunks = chunks_of(n_local)
    per = n_local // chunks
    ep_arg = lax.axis_index("ep").reshape(1).astype(jnp.int32)
    outgoing, cols = dispatch(
        core_arg, ep_arg, tokens_b, norm_gain[None], routes.T, route_weight.T, n_z, n_ep, n_local,
        per,
    )
    arrived = []
    for chunk in range(chunks):
        here = []
        for step in range(n_ep):
            piece = outgoing[chunk * n_ep + step].reshape(per, n_z * CAP, d_model)
            here.append(shift(piece, "ep", step) if step else piece)
        arrived.append((here, [swap_cores(p) for p in here]))

    all_weights = [gate_weight, up_weight, down_weight]
    weights = [load(all_weights, chunk * per, per, cols) for chunk in range(1, chunks)]
    steps = list(range(n_z))
    far, near = steps[n_z // 2 :], steps[: n_z // 2]
    own = (z_arg, q_own, q_other, query_gain[None], cosine, sine, out_weight, w_other)
    far_rows, first_part, joined = mix(*own, pieces, far, all_weights[:2], per)
    near_rows, last_part, _ = mix(*own, joined, near, all_weights[2:], per)
    weights = [[*first_part, *last_part], *weights]
    gathered = []
    for step, rows in zip(near + far, [*near_rows, *far_rows]):
        gathered.append(shift(rows, "z", step) if step else rows)
    mixed_out = add(*gathered)[0]

    backs = [[], []]
    for chunk in range(chunks):
        halves = 2 if chunk == chunks - 1 else 1
        keep, send = experts(*arrived[chunk], weights[chunk])
        for step in range(n_ep):
            result = add(keep[step], swap_cores(send[step]), halves=halves)
            for half in range(2):
                if half < halves:
                    piece = shift(result[half], "ep", step, back=True) if step else result[half]
                    piece = piece.reshape(-1, piece.shape[-1])
                backs[half].append(piece)
    parts = [[] for _ in range(n_z)]
    for half in range(2):
        width = d_model // 2
        rows = combine(z_arg, cols, backs[half], n_z, half * width, width)
        for step in range(n_z):
            parts[step].append(shift(rows[step], "z", step) if step else rows[step])
    return (mixed_out, join(parts))


def solution(mesh):
    n_ep, n_tp = mesh.shape["ep"], mesh.shape["tp"]
    fine = Mesh(mesh.devices.reshape(n_ep, n_tp // CORES, CORES), ("ep", "z", "core"))
    tp = ("z", "core")
    placed = (
        P("ep", tp),
        P("ep", None),
        P("ep", None),
        P(),
        P(),
        P(tp, None),
        P("ep", None),
        P(),
        P("ep", None),
        P("ep", None),
        P("ep", None, tp),
        P("ep", None, tp),
        P("ep", tp, None),
    )

    return jax.shard_map(
        on_device,
        mesh=fine,
        in_specs=placed,
        out_specs=(P(("ep", "z", "core"), None), P(("ep", "z", "core"), None)),
        check_vma=False,
    )
```

```python
import jax
import jax.numpy as jnp
from jax import lax
from jax.experimental import pallas as pl
from jax.experimental.pallas import tpu as pltpu
from jax.sharding import Mesh, PartitionSpec as P


HD = 128
KVH = 4
EXPERTS = 16
TOPK = 2
GRID_W = 64
CAP = 8
EPS = 1e-06
THETA = 10000.0
CORES = 2
IN_VMEM = pl.BlockSpec(memory_space=pltpu.VMEM)
IN_SMEM = pl.BlockSpec(memory_space=pltpu.SMEM)
SPLIT = 2
KEY_CHUNK = 1024
MIB = 1024 * 1024

F32 = jnp.float32
BF16 = jnp.bfloat16


def in_hbm(arrays):
    return [pltpu.with_memory_space_constraint(a, pltpu.HBM) for a in arrays]


def rope_tables(positions):
    n_freq = HD // 4
    row_pos = (positions // GRID_W).astype(F32)[:, None]
    col_pos = (positions % GRID_W).astype(F32)[:, None]
    lane = jnp.arange(HD, dtype=jnp.int32)
    inverse = THETA ** (-(lane % n_freq).astype(F32) / n_freq)
    angle = jnp.where(lane < HD // 2, row_pos, col_pos) * inverse
    sign = jnp.where((lane // n_freq) % 2 == 0, -1.0, 1.0).astype(F32)
    return jnp.cos(angle), jnp.sin(angle) * sign


def norm_turn(field, gain, cosine, sine):
    quarter = HD // 4
    mean = jnp.mean(field * field, axis=-1, keepdims=True)
    field = field * lax.rsqrt(mean + EPS) * gain
    lane = lax.broadcasted_iota(jnp.int32, field.shape, 1)
    partner = jnp.where(
        (lane // quarter) % 2 == 0,
        pltpu.roll(field, HD - quarter, 1),
        pltpu.roll(field, quarter, 1),
    )
    return field * cosine + partner * sine


def prepare_kernel(
    core_ref, head_ref, keys_ref, values_ref, q_ref, own_ref, gain_ref, cos_ref, sin_ref,
    kv_ref, send_ref, keep_ref,
):
    rows = cos_ref.shape[0]
    field = keys_ref[...].reshape(rows, HD).astype(F32)
    kv_ref[0] = norm_turn(field, gain_ref[...], cos_ref[...], sin_ref[...]).astype(BF16)
    kv_ref[1] = values_ref[...].reshape(rows, HD)
    send_ref[...] = q_ref[...].reshape(send_ref.shape)
    keep_ref[...] = own_ref[...].reshape(keep_ref.shape)


def prepare(core, head, keys, values, queries, gain, cosine, sine, n_z):
    rows, width = cosine.shape[0], queries.shape[-1]
    part = rows // n_z
    view = lambda a: a.reshape(n_z, CORES, part, a.shape[-1])
    picked = pl.BlockSpec((n_z, 1, part, HD), lambda i, c, h: (0, c[0], 0, h[0]))
    whole = lambda shape: pl.BlockSpec(shape, lambda i, c, h: (0,) * len(shape))
    return pl.pallas_call(
        prepare_kernel,
        grid_spec=pltpu.PrefetchScalarGridSpec(
            num_scalar_prefetch=2,
            grid=(1,),
            in_specs=[
                picked,
                picked,
                pl.BlockSpec((n_z, 1, part, width), lambda i, c, h: (0, 1 - c[0], 0, 0)),
                pl.BlockSpec((n_z, 1, part, width), lambda i, c, h: (0, c[0], 0, 0)),
                whole((1, HD)),
                whole((rows, HD)),
                whole((rows, HD)),
            ],
            out_specs=[IN_VMEM] * 3,
        ),
        out_shape=[
            jax.ShapeDtypeStruct((2, rows, HD), BF16),
            jax.ShapeDtypeStruct((n_z, part, width), BF16),
            jax.ShapeDtypeStruct((n_z, part, width), BF16),
        ],
        compiler_params=pltpu.CompilerParams(vmem_limit_bytes=8 * MIB),
        name="prepare",
    )(
        core, head, *in_hbm([view(keys), view(values), view(queries), view(queries), gain]),
        cosine, sine,
    )


def add_kernel(n_out, *refs):
    ins, outs = refs[:-n_out], refs[-n_out:]
    total = ins[0][...].astype(F32)
    for ref in ins[1:]:
        total = total + ref[...].astype(F32)
    width = outs[0].shape[-1]
    for n, ref in enumerate(outs):
        ref[...] = total[..., n * width : (n + 1) * width].astype(BF16)


def add(*arrays, halves=1):
    *lead, width = arrays[0].shape
    out = jax.ShapeDtypeStruct((*lead, width // halves), BF16)
    return pl.pallas_call(
        lambda *refs: add_kernel(halves, *refs),
        in_specs=[IN_VMEM] * len(arrays),
        out_specs=[IN_VMEM] * halves,
        out_shape=[out] * halves,
        compiler_params=pltpu.CompilerParams(vmem_limit_bytes=8 * MIB),
        name="add",
    )(*arrays)


def join_kernel(*refs):
    ins, out_ref = refs[:-1], refs[-1]
    width = ins[0].shape[-1]
    count = out_ref.shape[-1] // width
    for n in range(count):
        total = ins[n][...].astype(F32)
        for ref in ins[n + count :: count]:
            total = total + ref[...].astype(F32)
        out_ref[:, n * width : (n + 1) * width] = total.astype(BF16)


def join(parts):
    flat = [h for part in parts for h in part]
    rows, width = flat[0].shape
    return pl.pallas_call(
        join_kernel,
        in_specs=[IN_VMEM] * len(flat),
        out_specs=IN_VMEM,
        out_shape=jax.ShapeDtypeStruct((rows, width * len(parts[0])), BF16),
        compiler_params=pltpu.CompilerParams(vmem_limit_bytes=8 * MIB),
        name="join",
    )(*flat)


def weight_copies(sources, targets, first, sems, sem):
    copies = []
    for source, target in zip(sources, targets):
        per, rows, _ = target.shape
        cut = rows // SPLIT
        for expert in range(per):
            for n in range(SPLIT):
                part = pl.ds(n * cut, cut)
                copies.append(
                    pltpu.make_async_copy(
                        source.at[first + expert, part], target.at[expert, part], sems.at[sem]
                    )
                )
                sem += 1
    return copies


def load_kernel(first, after_ref, *refs):
    count = len(refs) // 2
    sources, targets, sems = refs[:count], refs[count:-1], refs[-1]
    copies = weight_copies(sources, targets, first, sems, 0)
    for copy in copies:
        copy.start()
    for copy in copies:
        copy.wait()


def load(weights, first, per, after):
    any_space = pl.BlockSpec(memory_space=pl.ANY)
    return pl.pallas_call(
        lambda *refs: load_kernel(first, *refs),
        in_specs=[any_space] * (1 + len(weights)),
        out_specs=[IN_VMEM] * len(weights),
        out_shape=[jax.ShapeDtypeStruct((per, *w.shape[1:]), BF16) for w in weights],
        scratch_shapes=[pltpu.SemaphoreType.DMA((len(weights) * per * SPLIT,))],
        compiler_params=pltpu.CompilerParams(vmem_limit_bytes=2 * MIB),
        name="load",
    )(after, *in_hbm(weights))


def mix_kernel(n_pieces, steps, n_loads, z_ref, q_own, q_other, gain_hbm, cos_ref, sin_ref, *rest):
    n_z = q_own.shape[0]
    w_other, w_hbm = rest[:2]
    pieces = rest[2 : 2 + n_pieces]
    sources = rest[2 + n_pieces : 2 + n_pieces + n_loads]
    outs = rest[2 + n_pieces + n_loads : -4]
    mixed_ref, w_own, gain_ref, sems = rest[-4:]
    n_out = len(steps)
    loaded = outs[n_out : n_out + n_loads]
    copies = [
        pltpu.make_async_copy(gain_hbm, gain_ref, sems.at[0]),
        pltpu.make_async_copy(w_hbm, w_own, sems.at[1]),
        *weight_copies(sources, loaded, 0, sems, 2),
    ]
    for copy in copies:
        copy.start()
    if len(outs) > n_out + n_loads:
        keys_ref, vals_ref = outs[n_out + n_loads :]
        row = 0
        for piece in pieces:
            rows = piece.shape[1]
            keys_ref[row : row + rows] = piece[0]
            vals_ref[row : row + rows, :HD] = piece[1]
            row += rows
        vals_ref[:, HD:] = jnp.ones((row, HD), BF16)
    else:
        keys_ref, vals_ref = pieces
        row = keys_ref.shape[0]
    factor = HD ** (-0.5) * 1.4426950408889634
    part = q_own.shape[1]
    heads = q_own.shape[-1] // HD
    n_chunks = max(1, row // KEY_CHUNK)
    cut = row // n_chunks
    tile = CORES * heads * part // 2

    copies[0].wait()
    copies[1].wait()

    def one(n, carry):
        block = peer(z_ref[0], n + steps[0], n_z)
        at = pl.multiple_of(block * part, 16)
        cosine, sine = cos_ref[pl.ds(at, part)], sin_ref[pl.ds(at, part)]
        queries = []
        for field in (q_own[block], q_other[block]):
            for head in range(heads):
                vec = field[:, head * HD : (head + 1) * HD].astype(F32)
                queries.append(norm_turn(vec, gain_ref[...], cosine, sine).astype(BF16))
        query = jnp.concatenate(queries, axis=0)
        tiles = [query[:tile], query[tile:]]
        score = lambda side, c: lax.dot_general(
            tiles[side], keys_ref[c * cut : (c + 1) * cut],
            (((1,), (1,)), ((), ())), preferred_element_type=F32,
        )
        work = [(c, side) for c in range(n_chunks) for side in range(2)]
        top, total = [None] * 2, [None] * 2
        scores = score(0, 0)
        for step, (c, side) in enumerate(work):
            after = score(work[step + 1][1], work[step + 1][0]) if step + 1 < len(work) else None
            here = jnp.max(scores, axis=1, keepdims=True)
            if c:
                here = jnp.maximum(top[side], here)
                shrink = jnp.exp2((top[side] - here) * factor)
            weights = jnp.exp2((scores - here) * factor).astype(BF16)
            part_sum = jnp.dot(
                weights, vals_ref[c * cut : (c + 1) * cut], preferred_element_type=F32
            )
            total[side] = total[side] * shrink + part_sum if c else part_sum
            top[side] = here
            scores = after
        mixed = None
        for side, weight in enumerate((w_own, w_other)):
            merged = (total[side][:, :HD] / total[side][:, HD:]).astype(BF16)
            merged = jnp.concatenate(
                [merged[h * part : (h + 1) * part] for h in range(heads)], axis=1
            )
            out = jnp.dot(merged, weight[...], preferred_element_type=F32)
            mixed = out if mixed is None else mixed + out
        mixed_ref[n] = mixed.astype(BF16)
        return carry

    lax.fori_loop(0, n_out, one, 0)
    for n, out_ref in enumerate(outs[:n_out]):
        out_ref[...] = mixed_ref[n]
    for copy in copies[2:]:
        copy.wait()


def mix(z_index, q_own, q_other, gain, cosine, sine, w_own, w_other, pieces, steps, loads, per):
    _, part, _ = q_own.shape
    d_model = w_own.shape[-1]
    joined = len(pieces) == 2
    length = pieces[0].shape[0] if joined else sum(p.shape[1] for p in pieces)
    whole = [] if joined else [(length, HD), (length, 2 * HD)]
    any_space = pl.BlockSpec(memory_space=pl.ANY)
    shapes = [(part, d_model)] * len(steps) + [(per, *w.shape[1:]) for w in loads] + whole
    outs = pl.pallas_call(
        lambda *refs: mix_kernel(len(pieces), steps, len(loads), *refs),
        in_specs=[IN_SMEM, IN_VMEM, IN_VMEM, any_space, IN_VMEM, IN_VMEM, IN_VMEM, any_space]
        + [IN_VMEM] * len(pieces)
        + [any_space] * len(loads),
        out_specs=[IN_VMEM] * len(shapes),
        out_shape=[jax.ShapeDtypeStruct(shape, BF16) for shape in shapes],
        scratch_shapes=[
            pltpu.VMEM((len(steps), part, d_model), BF16),
            pltpu.VMEM(w_own.shape, BF16),
            pltpu.VMEM(gain.shape, F32),
            pltpu.SemaphoreType.DMA((2 + len(loads) * per * SPLIT,)),
        ],
        compiler_params=pltpu.CompilerParams(vmem_limit_bytes=10 * MIB),
        name="mix",
    )(
        z_index, q_own, q_other, *in_hbm([gain]), cosine, sine, w_other, *in_hbm([w_own]),
        *pieces, *in_hbm(loads),
    )
    at = len(steps)
    return outs[:at], outs[at : at + len(loads)], outs[at + len(loads) :]


def block_of(index, block, count):
    found = jnp.zeros_like(index)
    for n in range(1, count):
        found = found + (index >= n * block).astype(jnp.int32)
    return found


def dispatch_kernel(
    n_ep, n_local, per, core_ref, ep_ref, tokens_ref, gain_ref, routes_ref, weight_ref, *rest
):
    out_refs, cols_ref = rest[:-1], rest[-1]
    n_z, _, block, d_model = tokens_ref.shape
    rows, local_rows = n_z * block, routes_ref.shape[1]
    iota = lambda shape, dim: lax.broadcasted_iota(jnp.int32, shape, dim)
    exact = dict(preferred_element_type=F32, precision=lax.Precision.HIGHEST)

    lane = iota((local_rows, rows), 1)
    lane_block = block_of(lane, block, n_z)
    source = lane + (lane_block * (CORES - 1) + core_ref[0]) * block
    select = (iota((local_rows, rows), 0) == source).astype(F32)
    chosen = jnp.dot(routes_ref[...].astype(F32), select, **exact)
    chosen = (chosen + 0.5).astype(jnp.int32)
    weight = jnp.dot(weight_ref[...], select, **exact)

    shape = (EXPERTS, rows)
    expert = iota(shape, 0)
    hot = [expert == chosen[k : k + 1] for k in range(TOPK)]
    either = hot[0]
    for one in hot[1:]:
        either = either | one
    square = (rows, rows)
    above, across = iota(square, 0), iota(square, 1)
    first = block_of(across, block, n_z) * block
    earlier = ((above < across) & (above >= first)).astype(F32).astype(BF16)
    count = jnp.dot(either.astype(F32).astype(BF16), earlier, preferred_element_type=F32)
    owner = block_of(expert, n_local, n_ep)
    if n_ep & (n_ep - 1) == 0:
        ahead = owner ^ ep_ref[0]
    else:
        ahead = owner - ep_ref[0]
        ahead = jnp.where(ahead < 0, ahead + n_ep, ahead)
    local = expert - owner * n_local
    turn = block_of(local, per, n_local // per)
    place = ((turn * n_ep + ahead) * per + local - turn * per) * (n_z * CAP)
    place = place + block_of(iota(shape, 1), block, n_z) * CAP + (count + 0.5).astype(jnp.int32)
    slots = [jnp.sum(jnp.where(h, place, 0), axis=0, keepdims=True) for h in hot]

    total = jnp.sum(weight, axis=0, keepdims=True)
    table = [s.astype(F32) for s in slots] + [weight[k : k + 1] / total for k in range(TOPK)]
    lines = iota((8, rows), 0)
    stacked = jnp.zeros((8, rows), F32)
    for n, line in enumerate(table):
        stacked = jnp.where(lines == n, line, stacked)
    same = (above == across).astype(F32)
    cols_ref[...] = lax.dot_general(same, stacked, (((1,), (1,)), ((), ())), **exact)

    field = tokens_ref[...].reshape(rows, d_model).astype(F32)
    mean = jnp.mean(field * field, axis=-1, keepdims=True)
    normed = (field * lax.rsqrt(mean + EPS) * gain_ref[...]).astype(BF16)
    n_slots = out_refs[0].shape[0]
    for piece, out_ref in enumerate(out_refs):
        slot = iota((n_slots, rows), 0) + piece * n_slots
        picked = slot == slots[0]
        for one in slots[1:]:
            picked = picked | (slot == one)
        picked = picked.astype(F32).astype(BF16)
        out_ref[...] = jnp.dot(picked, normed, preferred_element_type=F32).astype(BF16)


def dispatch(core, ep, tokens, gain, routes, weight, n_z, n_ep, n_local, per):
    local_rows, d_model = tokens.shape
    block = local_rows // (n_z * CORES)
    n_slots = per * n_z * CAP
    n_out = n_ep * (n_local // per)
    whole = lambda a: pl.BlockSpec(a.shape, lambda i, c, e: (0,) * a.ndim)
    outs = pl.pallas_call(
        lambda *refs: dispatch_kernel(n_ep, n_local, per, *refs),
        grid_spec=pltpu.PrefetchScalarGridSpec(
            num_scalar_prefetch=2,
            grid=(1,),
            in_specs=[
                pl.BlockSpec((n_z, 1, block, d_model), lambda i, c, e: (0, c[0], 0, 0)),
                whole(gain),
                whole(routes),
                whole(weight),
            ],
            out_specs=[IN_VMEM] * (n_out + 1),
        ),
        out_shape=[jax.ShapeDtypeStruct((n_slots, d_model), BF16)] * n_out
        + [jax.ShapeDtypeStruct((n_z * block, 8), F32)],
        compiler_params=pltpu.CompilerParams(vmem_limit_bytes=16 * MIB),
        name="dispatch",
    )(core, ep, *in_hbm([tokens.reshape(n_z, CORES, block, d_model), gain, routes, weight]))
    return outs[:n_out], outs[n_out]


def expert_kernel(n_in, group, *refs):
    ins, (gate_ref, up_ref, down_ref) = refs[:n_in], refs[n_in : n_in + 3]
    outs = refs[n_in + 3 :]
    per, rows, _ = outs[0].shape
    for expert in range(per):
        for start in range(0, len(ins), group):
            field = [ref[expert] for ref in ins[start : start + group]]
            field = jnp.concatenate(field, axis=0)
            gate = jnp.dot(field, gate_ref[expert], preferred_element_type=F32)
            up = jnp.dot(field, up_ref[expert], preferred_element_type=F32)
            hidden = (gate / (1.0 + jnp.exp(-gate)) * up).astype(BF16)
            result = jnp.dot(hidden, down_ref[expert], preferred_element_type=F32)
            for n, ref in enumerate(outs[start : start + group]):
                ref[expert] = result[n * rows : (n + 1) * rows].astype(BF16)


def experts(own, other, weights):
    pieces = [*own, *other]
    _, rows, d_model = pieces[0].shape
    per = weights[0].shape[0]
    group = min(len(pieces), max(1, 256 // rows))
    outs = pl.pallas_call(
        lambda *refs: expert_kernel(len(pieces), group, *refs),
        in_specs=[IN_VMEM] * (len(pieces) + 3),
        out_specs=[IN_VMEM] * len(pieces),
        out_shape=[jax.ShapeDtypeStruct((per, rows, d_model), BF16)] * len(pieces),
        compiler_params=pltpu.CompilerParams(vmem_limit_bytes=10 * MIB),
        name="experts",
    )(*pieces, *weights)
    return outs[: len(own)], outs[len(own) :]


def combine_kernel(n_back, at, z_ref, cols_ref, *rest):
    back_refs, out_refs, total_ref = rest[:n_back], rest[n_back:-1], rest[-1]
    rows = cols_ref.shape[0]
    width = total_ref.shape[-1]
    back = [ref[:, at : at + width] if ref.shape[-1] > width else ref[...] for ref in back_refs]
    back = jnp.concatenate(back, axis=0)
    slot = lax.broadcasted_iota(jnp.int32, (rows, back.shape[0]), 1)
    matrix = jnp.zeros(slot.shape, F32)
    for k in range(TOPK):
        own = (cols_ref[:, k : k + 1] + 0.5).astype(jnp.int32)
        share = cols_ref[:, TOPK + k : TOPK + k + 1]
        matrix = matrix + jnp.where(slot == own, share, 0.0)
    high = matrix.astype(BF16)
    low = (matrix - high.astype(F32)).astype(BF16)
    both = jnp.dot(jnp.concatenate([high, low], axis=0), back, preferred_element_type=F32)
    total_ref[...] = (both[:rows] + both[rows:]).reshape(total_ref.shape)
    n_z = len(out_refs)
    for n, out_ref in enumerate(out_refs):
        out_ref[...] = total_ref[peer(z_ref[0], n, n_z)].astype(BF16)


def combine(z_index, cols, backs, n_z, at, width):
    rows = cols.shape[0]
    return pl.pallas_call(
        lambda *refs: combine_kernel(len(backs), at, *refs),
        in_specs=[IN_SMEM] + [IN_VMEM] * (1 + len(backs)),
        out_specs=[IN_VMEM] * n_z,
        out_shape=[jax.ShapeDtypeStruct((rows // n_z, width), BF16)] * n_z,
        scratch_shapes=[pltpu.VMEM((n_z, rows // n_z, width), F32)],
        compiler_params=pltpu.CompilerParams(vmem_limit_bytes=24 * MIB),
        name="combine",
    )(z_index, cols, *backs)


def chunks_of(n_local):
    return 2 if n_local % 2 == 0 else 1


def peer(own, step, n):
    return own ^ step if n & (n - 1) == 0 else lax.rem(own + step, n)


def shift(a, axis, step, back=False):
    n = lax.axis_size(axis)
    if n & (n - 1) == 0:
        pairs = [(i, i ^ step) for i in range(n)]
    else:
        pairs = [(i, (i - step if back else i + step) % n) for i in range(n)]
    return lax.ppermute(a, axis, pairs)


def swap_cores(a):
    return lax.ppermute(a, "core", [(i, CORES - 1 - i) for i in range(CORES)])


def on_device(
    queries,
    keys,
    values,
    query_gain,
    key_gain,
    out_weight,
    tokens_b,
    norm_gain,
    routes,
    route_weight,
    gate_weight,
    up_weight,
    down_weight,
):
    n_ep, n_z = lax.axis_size("ep"), lax.axis_size("z")
    core, z_index = lax.axis_index("core"), lax.axis_index("z")
    core_arg = core.reshape(1).astype(jnp.int32)
    z_arg = z_index.reshape(1).astype(jnp.int32)
    n_rows, width = queries.shape
    d_model = tokens_b.shape[-1]
    heads = width // HD
    n_heads = heads * n_z * CORES

    part = n_rows // (n_z * CORES)
    offsets = (
        jnp.arange(n_z, dtype=jnp.int32)[:, None] * (CORES * part)
        + core * part
        + jnp.arange(part, dtype=jnp.int32)[None, :]
    ).reshape(-1)
    cosine, sine = rope_tables(lax.axis_index("ep") * n_rows + offsets)
    kv_head = ((z_index * CORES + core) * heads // (n_heads // KVH)).reshape(1).astype(jnp.int32)
    own_kv, q_send, q_own = prepare(
        core_arg, kv_head, keys, values, queries, key_gain[None], cosine, sine, n_z
    )
    pieces = [own_kv]
    for step in range(1, n_ep):
        pieces.append(shift(own_kv, "ep", step))
    pieces = pieces + [swap_cores(p) for p in pieces]

    q_other = swap_cores(q_send)
    w_other = swap_cores(out_weight)

    n_local = gate_weight.shape[0]
    chunks = chunks_of(n_local)
    per = n_local // chunks
    ep_arg = lax.axis_index("ep").reshape(1).astype(jnp.int32)
    outgoing, cols = dispatch(
        core_arg, ep_arg, tokens_b, norm_gain[None], routes.T, route_weight.T, n_z, n_ep, n_local,
        per,
    )
    arrived = []
    for chunk in range(chunks):
        here = []
        for step in range(n_ep):
            piece = outgoing[chunk * n_ep + step].reshape(per, n_z * CAP, d_model)
            here.append(shift(piece, "ep", step) if step else piece)
        arrived.append((here, [swap_cores(p) for p in here]))

    all_weights = [gate_weight, up_weight, down_weight]
    weights = [load(all_weights, chunk * per, per, cols) for chunk in range(1, chunks)]
    last_part = load(all_weights[2:], 0, per, cols)
    steps = list(range(n_z))
    far, near = steps[n_z // 2 :], steps[: n_z // 2]
    own = (z_arg, q_own, q_other, query_gain[None], cosine, sine, out_weight, w_other)
    far_rows, first_part, joined = mix(*own, pieces, far, all_weights[:2], per)
    near_rows, _, _ = mix(*own, joined, near, [], per)
    weights = [[*first_part, *last_part], *weights]
    gathered = []
    for step, rows in zip(near + far, [*near_rows, *far_rows]):
        gathered.append(shift(rows, "z", step) if step else rows)
    mixed_out = add(*gathered)[0]

    backs = [[], []]
    for chunk in range(chunks):
        halves = 2 if chunk == chunks - 1 else 1
        keep, send = experts(*arrived[chunk], weights[chunk])
        for step in range(n_ep):
            result = add(keep[step], swap_cores(send[step]), halves=halves)
            for half in range(2):
                if half < halves:
                    piece = shift(result[half], "ep", step, back=True) if step else result[half]
                    piece = piece.reshape(-1, piece.shape[-1])
                backs[half].append(piece)
    parts = [[] for _ in range(n_z)]
    for half in range(2):
        width = d_model // 2
        rows = combine(z_arg, cols, backs[half], n_z, half * width, width)
        for step in range(n_z):
            parts[step].append(shift(rows[step], "z", step) if step else rows[step])
    return (mixed_out, join(parts))


def solution(mesh):
    n_ep, n_tp = mesh.shape["ep"], mesh.shape["tp"]
    fine = Mesh(mesh.devices.reshape(n_ep, n_tp // CORES, CORES), ("ep", "z", "core"))
    tp = ("z", "core")
    placed = (
        P("ep", tp),
        P("ep", None),
        P("ep", None),
        P(),
        P(),
        P(tp, None),
        P("ep", None),
        P(),
        P("ep", None),
        P("ep", None),
        P("ep", None, tp),
        P("ep", None, tp),
        P("ep", tp, None),
    )

    return jax.shard_map(
        on_device,
        mesh=fine,
        in_specs=placed,
        out_specs=(P(("ep", "z", "core"), None), P(("ep", "z", "core"), None)),
        check_vma=False,
    )
```
